32 devices in a mesh: vp: 8 (over z, x), dp: 4 (over y, core).
Axes of the slice: x: 2, y: 2, z: 4, core: 2. Of those that a mesh axis runs over, the one named last changes fastest.
Arguments:
- stream: bfloat16 [1024, 2048], P(('dp', 'vp')), may hold values from -60 to 60
- hidden: bfloat16 [1024, 5632], P('dp', 'vp'), may hold values from -6 to 6
- w_down: bfloat16 [5632, 2048], P(None, 'vp'), may hold values from -0.078125 to 0.078125
- final_gain: float32 [2048], replicated, may hold values from 0.1 to 1.9
- vocab: bfloat16 [2048, 32768], P(None, 'vp'), may hold values from -2 to 200
- vocab_bias: float32 [32768], P('vp'), may hold values from -5 to 5
- targets: int32 [1024], P('dp'), may hold values from 0 to 32767
Outputs:
- losses: float32 [1024], P(('dp', 'vp'))
- grad_input: float32 [1024, 2048], P(('dp', 'vp'))
- grad_vocab: float32 [2048, 32768], P('dp', 'vp')
The draws below stay inside these ranges and needn't reach their ends.
All inputs are finite; a program needn't handle non-finite values.
Results may differ from the reference program's by a relative error of at most 0.02.
Values may be sent and summed in bfloat16 or wider, within the bound.
A program may use at most 128 MiB of HBM per device.

```python
import math
import jax
import jax.numpy as jnp
import numpy as np
from jax import lax

D = 2048
FF = 5632
VOCAB = 32768
TOK_GROUP = 256
TOKENS = 1024
COLS_DEV = 4096


def draw_stream(key, part):
    ramp = 3.0 ** (jnp.arange(D, dtype=jnp.float32) / (D - 1))
    base = jnp.clip(jax.random.normal(key, (TOKENS, D), jnp.float32), -6.0, 6.0)
    values = base * ramp
    return values.astype(jnp.bfloat16)


def draw_vocab(key, part):
    base = jnp.clip(jax.random.normal(key, (D, VOCAB), jnp.float32), -6.0, 6.0) * (2.5 / math.sqrt(D))
    return base.astype(jnp.bfloat16)


def draw_vocab_bias(key, part):
    shards = VOCAB // COLS_DEV
    shard = (jnp.arange(VOCAB, dtype=jnp.int32) // COLS_DEV).astype(jnp.float32)
    ramp = 2.0 * shard / max(shards - 1, 1) - 1.0
    noise = jnp.clip(jax.random.normal(key, (VOCAB,), jnp.float32), -4.0, 4.0)
    return 0.5 * noise + ramp


def with_ends(result, own_key, least, largest):
    place = [jax.random.randint(jax.random.fold_in(own_key, axis), (), 0, length) for axis, length in enumerate(result.shape)]
    widest = result.shape.index(max(result.shape))
    next_to = place[:widest] + [(place[widest] + 1) % result.shape[widest]] + place[widest + 1:]
    return result.at[tuple(place)].set(least).at[tuple(next_to)].set(largest)


def steps_of(key, shape, cuts, low, high):
    gain, own = 1.0, jax.random.fold_in(key, 6)
    for position, shards_of in cuts:
        draws = jnp.exp(jax.random.uniform(jax.random.fold_in(own, position), (shards_of,), jnp.float32, low / len(cuts), high / len(cuts)))
        gain = gain * jnp.repeat(draws, shape[position] // shards_of).reshape([-1 if axis == position else 1 for axis in range(len(shape))])
    return gain


def rank_table(amount, lean):
    portions = [(1 << 20) // math.isqrt(standing ** lean) + 1 for standing in range(1, amount + 1)]
    width = 1 + sum(portions) // (1 << 30)
    return np.cumsum(np.array([max(1, weight // width) for weight in portions]))


def ranked_ids(own_key, dims, count, lean):
    listing = rank_table(count, lean)
    pick = jax.random.randint(jax.random.fold_in(own_key, 1), dims, 0, int(listing[count - 1]))
    standing = jnp.searchsorted(jnp.asarray(listing, jnp.int32), pick, side="right")
    return jax.random.permutation(jax.random.fold_in(own_key, 2), count)[standing].astype(jnp.int32)


def centred(own_key, dims, deviation, reach, split=(), kind=jnp.bfloat16):
    result = deviation * jax.random.normal(own_key, dims, jnp.float32)
    if split:
        result = result * steps_of(own_key, dims, split, -0.22, 0.18)
    return jnp.clip(result, -reach, reach).astype(kind)


def setup_inputs(seed: int = 0) -> dict:
    key_list = jax.random.split(jax.random.key(seed), 8)
    return {
        "stream": draw_stream(jax.random.fold_in(key_list[7], 71), 0),
        "hidden": centred(key_list[1], (TOKENS, FF), 1.0, 6.0, ((0, 4), (1, 8))),
        "w_down": centred(key_list[2], (FF, D), FF ** -0.5, 0.078125, ((1, 8),)),
        "final_gain": jnp.clip(1.0 + 0.18 * jax.random.normal(key_list[3], (D,), jnp.float32), 0.1, 1.9),
        "vocab": draw_vocab(jax.random.fold_in(key_list[7], 71), 0),
        "vocab_bias": draw_vocab_bias(jax.random.fold_in(key_list[7], 71), 0),
        "targets": with_ends(ranked_ids(key_list[6], (TOKENS,), VOCAB, 2), jax.random.fold_in(key_list[6], 3), 0, VOCAB - 1).astype(jnp.int32),
    }


norm_eps = 1e-06
zloss_weight = 0.001

def reference(stream, hidden, w_down, final_gain, vocab, vocab_bias, targets):
    proj = jnp.dot(hidden, w_down, preferred_element_type=jnp.float32)
    normin = (stream.astype(jnp.float32) + proj).astype(jnp.bfloat16)
    values = normin.astype(jnp.float32)
    inv = lax.rsqrt(lax.optimization_barrier(jnp.mean(values * values, axis=1, keepdims=True)) + norm_eps)
    normed = (values * inv * final_gain).astype(jnp.bfloat16)
    groups = TOKENS // TOK_GROUP
    normed_blocks = normed.reshape(groups, TOK_GROUP, D)
    target_blocks = targets.reshape(groups, TOK_GROUP)

    def one_group(carry, inputs):
        rows, goal = inputs
        scores = jnp.dot(rows, vocab, preferred_element_type=jnp.float32) + vocab_bias
        top = lax.optimization_barrier(jnp.max(scores, axis=1))
        lse = top + jnp.log(lax.optimization_barrier(jnp.sum(jnp.exp(scores - top[:, None]), axis=1)))
        hit = lax.broadcasted_iota(jnp.int32, (TOK_GROUP, VOCAB), 1) == goal[:, None]
        target_score = lax.optimization_barrier(jnp.sum(jnp.where(hit, scores, 0.0), axis=1))
        losses = lse - target_score + zloss_weight * lse * lse
        probs = jnp.exp(scores - lse[:, None])
        dscore = (probs * (1.0 + 2.0 * zloss_weight * lse)[:, None] - jnp.where(hit, 1.0, 0.0)).astype(jnp.bfloat16)
        drows = jnp.dot(dscore, vocab.T, preferred_element_type=jnp.float32)
        carry = carry + jnp.dot(rows.T, dscore, preferred_element_type=jnp.float32)
        return (carry, (losses, drows))
    grad_vocab, (losses, drows) = lax.scan(one_group, jnp.zeros((D, VOCAB), jnp.float32), (normed_blocks, target_blocks))
    dnormed = drows.reshape(TOKENS, D)
    scaled = dnormed * final_gain
    grad_input = inv * (scaled - values * inv * inv * lax.optimization_barrier(jnp.mean(values * scaled, axis=1, keepdims=True)))
    return (losses.reshape(TOKENS), grad_input, grad_vocab)
```

```python
import functools

import jax
import jax.numpy as jnp
from jax import lax
from jax.experimental import pallas as pl
from jax.experimental.pallas import tpu as pltpu
from jax.sharding import PartitionSpec as P

norm_eps = 1e-06
zloss_weight = 0.001


def combined_all(value, axis, join):
    pieces = jax.tree.map(lambda part: lax.all_gather(part, axis), value)
    head = jax.tree.map(lambda part: part[0], pieces)
    tail = jax.tree.map(lambda part: part[1:], pieces)
    total, _ = lax.scan(lambda total, section: (join(total, section), None), head, tail)
    return total


def combine_stats(first, second):
    top = jnp.maximum(first[0], second[0])
    total = first[1] * jnp.exp(first[0] - top) + second[1] * jnp.exp(second[0] - top)
    return (top, total, first[2] + second[2])


def body(stream, hidden, w_down, final_gain, vocab, vocab_bias, targets):
    rows_dev = stream.shape[0]
    width = stream.shape[1]
    group = targets.shape[0]
    mine = lax.axis_index("vp")
    feat_cols = w_down.shape[1]
    proj = jnp.dot(
        lax.all_gather(hidden, "vp", axis=1, tiled=True), w_down, preferred_element_type=jnp.float32
    )
    stream_cols = lax.all_to_all(stream, "vp", split_axis=1, concat_axis=0, tiled=True)
    normin_cols = (stream_cols.astype(jnp.float32) + proj).astype(jnp.bfloat16)
    col_values = normin_cols.astype(jnp.float32)
    square_total = lax.psum(jnp.sum(col_values * col_values, axis=1), "vp")
    inv_group = lax.rsqrt(square_total / width + norm_eps)
    gain_cols = lax.dynamic_slice_in_dim(final_gain, mine * feat_cols, feat_cols)
    normed_cols = (col_values * inv_group[:, None] * gain_cols).astype(jnp.bfloat16)
    normed = lax.all_gather(normed_cols, "vp", axis=1, tiled=True)
    normin = lax.all_to_all(normin_cols, "vp", split_axis=0, concat_axis=1, tiled=True)
    values = normin.astype(jnp.float32)
    inv = lax.rsqrt(jnp.mean(values * values, axis=1, keepdims=True) + norm_eps)
    ncols = vocab.shape[1]
    scores = jnp.dot(normed, vocab, preferred_element_type=jnp.float32) + vocab_bias
    local_top = jnp.max(scores, axis=1)
    local_total = jnp.sum(jnp.exp(scores - local_top[:, None]), axis=1)
    column_ids = lax.broadcasted_iota(jnp.int32, (group, ncols), 1) + mine * ncols
    hit = column_ids == targets[:, None]
    local_target = jnp.sum(jnp.where(hit, scores, 0.0), axis=1)
    top, total, target_score = combined_all(
        (local_top, local_total, local_target), "vp", combine_stats
    )
    lse = top + jnp.log(total)
    group_losses = lse - target_score + zloss_weight * lse * lse
    losses = lax.dynamic_slice_in_dim(group_losses, mine * rows_dev, rows_dev)
    probs = jnp.exp(scores - lse[:, None])
    dscore = (probs * (1.0 + 2.0 * zloss_weight * lse)[:, None] - jnp.where(hit, 1.0, 0.0)).astype(
        jnp.bfloat16
    )
    feat_group = width // lax.axis_size("dp")
    feat_start = lax.axis_index("dp") * feat_group
    rows_slice = lax.dynamic_slice_in_dim(
        lax.all_gather(normed, "dp", axis=0, tiled=True), feat_start, feat_group, 1
    )
    grad_vocab = lax.dot_general(
        rows_slice,
        lax.all_gather(dscore, "dp", axis=0, tiled=True),
        (((0,), (0,)), ((), ())),
        preferred_element_type=jnp.float32,
    )
    row_term = lax.dot_general(
        dscore, vocab, (((1,), (1,)), ((), ())), preferred_element_type=jnp.float32
    )
    row_parts = lax.all_to_all(
        row_term[:, None, :].astype(jnp.bfloat16), "vp", split_axis=0, concat_axis=1, tiled=True
    ).astype(jnp.float32)
    dnormed = jnp.sum(row_parts, axis=1)
    scaled = dnormed * final_gain
    grad_input = inv * (
        scaled - values * inv * inv * jnp.mean(values * scaled, axis=1, keepdims=True)
    )
    return (losses, grad_input, grad_vocab)


MESH = pl.DeviceIdType.MESH
UNIT_PARTS = 2
NORM_PARTS = 4
TILE = 512
BLOCK = 512


def send(src, dst, send_sem, recv_sem, vp, dp):
    return pltpu.make_async_remote_copy(
        src_ref=src,
        dst_ref=dst,
        send_sem=send_sem,
        recv_sem=recv_sem,
        device_id={"vp": vp, "dp": dp},
        device_id_type=MESH,
    )


def gather(n, me, dp, parts, own, place, bulk, sems, extra, first, use):
    line = n // 2
    here = me // 2
    side = me - 2 * here
    other = me + 1 - 2 * side
    turn = parts // 2
    send_sem, recv_sem = sems
    targets = {0: other, 1: me + 2, 2: me - 2}
    sent = []

    def copy(way, slot, part, src=None):
        return send(
            place(slot, part) if src is None else src,
            place(slot, part),
            send_sem.at[way],
            recv_sem.at[slot, part],
            targets[way],
            dp,
        )

    def holds(conditions, row):
        return functools.reduce(lambda a, b: a & b, [test(row) for test in conditions])

    def when(conditions, action):
        if conditions:
            pl.when(holds(conditions, here))(action)
        else:
            action()

    def put(outer, inner, way, slot, part, src=None):
        when(inner, lambda: copy(way, slot, part, src).start())
        sent.append((outer + inner, way))

    def live(step):
        if step == 0:
            return []
        return [lambda row: (row + step < line) & (row + step >= 0)]

    def ends(step):
        return [lambda row: row + step == (line - 1 if step > 0 else 0)]

    def inside(step):
        return [lambda row: row + step != (line - 1 if step > 0 else 0)]

    up, down = [lambda row: row < line - 1], [lambda row: row > 0]

    for part in range(parts):
        put([], [], 0, me, part, own(part))
        put([], up, 1, me, part, own(part))
        put([], down, 2, me, part, own(part))
        extra(me, part)
    first()

    def straight(k, part, step, way):
        slot = me + 2 * step
        outer = live(step)

        def receive():
            copy(0, slot, part).wait_recv()
            put(outer, up if way == 1 else down, way, slot, part)
            put(outer, inside(step) if part >= turn else [], 0, slot, part)
            extra(slot, part)

        when(outer, receive)

    def routed(k):
        for step, way in ((-k, 1), (k, 2)):
            slot = other + 2 * step
            outer = live(step) + ends(step)

            def receive(slot=slot, outer=outer, way=way):
                for part in range(turn, parts):
                    copy(0, slot, part).wait_recv()
                    put(outer, up if way == 1 else down, way, slot, part)
                    extra(slot, part)

            when(outer, receive)

    def crossed(k):
        for part in range(parts):
            for step in (-k, k) if k else (0,):
                slot = other + 2 * step
                outer = live(step)
                if k and part >= turn:
                    outer = outer + inside(step)

                def receive(slot=slot, part=part):
                    copy(0, slot, part).wait_recv()
                    extra(slot, part)

                when(outer, receive)
                if k == 0 and part >= turn:
                    put([], [lambda row: row == 0] + up, 1, slot, part)
                    put([], [lambda row: row == line - 1] + down, 2, slot, part)

    def used(base, k):
        for step in (-k, k) if k else (0,):
            when(live(step), lambda step=step: use(base + 2 * step))

    for k in range(1, line):
        for part in range(parts):
            straight(k, part, -k, 1)
            straight(k, part, k, 2)
        if k > 1:
            routed(k - 1)
        crossed(k - 1)
        used(me, k)
        used(other, k - 1)
    if line > 1:
        routed(line - 1)
    crossed(line - 1)
    used(other, line - 1)

    def finish():
        for way in range(3):
            for row in range(line):
                count = sum(1 for tests, which in sent if which == way and (not tests or holds(tests, row)))
                if count:
                    pl.when(here == row)(lambda: await_bytes(bulk(count), send_sem.at[way]))

    return finish


def await_bytes(ref, sem):
    pltpu.make_async_copy(ref, ref, sem).wait()


def head_kernel(
    n,
    hidden,
    w_down_in,
    stream_in,
    gain_in,
    vocab,
    bias_in,
    targets_in,
    loss_out,
    input_out,
    score_out,
    flip_out,
    w_down,
    stream,
    gain,
    bias,
    targets,
    loss_buf,
    input_buf,
    flip_buf,
    units,
    stream_cols,
    normin,
    normed,
    words,
    scores,
    tops,
    lanes,
    stats,
    goals,
    total,
    dscore,
    slices,
    terms,
    crossing,
    sums,
    landed,
    unit_send,
    unit_recv,
    norm_send,
    norm_recv,
    stream_send,
    stream_recv,
    twin_send,
    twin_recv,
    stat_send,
    stat_recv,
    score_send,
    score_recv,
    slice_send,
    slice_recv,
    cross_send,
    cross_recv,
    term_send,
    term_recv,
    load_sem,
    keep_sem,
    out_sem,
):
    me = lax.axis_index("vp")
    dp = lax.axis_index("dp")
    twin = lax.rem(dp + 2, 4)
    core = lax.rem(dp, 2)
    sibling = dp + 1 - 2 * core
    line = n // 2
    place = me // 2
    side = me - 2 * place
    other = me + 1 - 2 * side
    depth, group = hidden.shape
    width = gain.shape[1]
    feats = stream_cols.shape[1]
    rows_dev = stream.shape[0]
    ncols = bias.shape[1]
    own_feats = slices.shape[1]
    half = group // NORM_PARTS
    piece = depth // UNIT_PARTS

    barrier = pltpu.get_barrier_semaphore()

    def greet(j, _):
        peer = lax.rem(me + j, n)
        pl.semaphore_signal(barrier, 1, device_id={"vp": peer, "dp": dp}, device_id_type=MESH)
        pl.semaphore_signal(barrier, 1, device_id={"vp": peer, "dp": twin}, device_id_type=MESH)
        return 0

    lax.fori_loop(1, n, greet, 0)
    pl.semaphore_signal(barrier, 1, device_id={"vp": me, "dp": twin}, device_id_type=MESH)
    pl.semaphore_signal(barrier, 1, device_id={"vp": me, "dp": sibling}, device_id_type=MESH)

    def brought(at, src, dst):
        return pltpu.make_async_copy(src, dst, load_sem.at[at])

    bring = brought(0, hidden, units.at[pl.ds(pl.multiple_of(me * depth, 16), depth), :])
    bring_stream = brought(1, stream_in, stream)
    bring_down = brought(2, w_down_in, w_down)
    bring_targets = brought(3, targets_in, targets)
    bring_gain = brought(4, gain_in, gain)
    bring_bias = brought(5, bias_in, bias)
    load = brought(6, vocab, words)
    for copy in (bring, bring_stream, bring_down, bring_targets, bring_gain, bring_bias, load):
        copy.start()
    pl.semaphore_wait(barrier, 2 * n)

    def stream_copy(j):
        peer = lax.rem(me + j, n)
        return send(
            stream.at[:, pl.ds(pl.multiple_of(peer * feats, 128), feats)],
            stream_cols.at[pl.ds(pl.multiple_of(me * rows_dev, rows_dev), rows_dev), :],
            stream_send,
            stream_recv,
            peer,
            dp,
        )

    def start_stream(j, _):
        stream_copy(j).start()
        return 0

    def place_units(slot, part):
        return units.at[pl.ds(pl.multiple_of(slot * depth + part * piece, 16), piece), :]

    def product(slot):
        rows = pl.ds(pl.multiple_of(slot * depth, 16), depth)
        return lax.dot_general(
            units[rows, :],
            w_down[rows, :],
            (((0,), (0,)), ((), ())),
            preferred_element_type=jnp.float32,
        )

    def open_units():
        bring_stream.wait()
        lax.fori_loop(1, n, start_stream, 0)
        stream_cols[pl.ds(pl.multiple_of(me * rows_dev, rows_dev), rows_dev), :] = stream[
            :, pl.ds(pl.multiple_of(me * feats, 128), feats)
        ]
        bring_targets.wait()
        goals[...] = jnp.transpose(
            jnp.broadcast_to(targets[...].astype(jnp.float32), (128, group))
        )
        bring_down.wait()
        total[...] = product(me)

    def project(slot):
        total[...] += product(slot)

    bring.wait()
    finish_units = gather(
        n,
        me,
        dp,
        UNIT_PARTS,
        lambda part: place_units(me, part),
        place_units,
        lambda count: units.at[pl.ds(0, count * piece), :],
        (unit_send, unit_recv),
        lambda slot, part: None,
        open_units,
        project,
    )
    streamed = stream_cols.at[pl.ds(0, (n - 1) * rows_dev), :]
    await_bytes(streamed, stream_recv)
    await_bytes(streamed, stream_send)

    def cols_of(slot):
        return pl.ds(pl.multiple_of(slot * feats, 128), feats)

    normin[0, :, cols_of(me)] = (stream_cols[...].astype(jnp.float32) + total[...]).astype(jnp.bfloat16)

    def twin_copy(slot, part):
        rows = pl.ds(part * half, half)
        return send(
            normin.at[0, rows, cols_of(slot)],
            normin.at[1, rows, cols_of(slot)],
            twin_send,
            twin_recv,
            me,
            twin,
        )

    def place_norm(slot, part):
        return normin.at[0, pl.ds(part * half, half), cols_of(slot)]

    def open_norm():
        bring_gain.wait()
        bring_bias.wait()
        tops[...] = jnp.full(tops.shape, -jnp.inf, jnp.float32)

    finish_norm = gather(
        n,
        me,
        dp,
        NORM_PARTS,
        lambda part: place_norm(me, part),
        place_norm,
        lambda count: scores.at[0, pl.ds(0, count * half // 8), pl.ds(0, 4 * feats)],
        (norm_send, norm_recv),
        lambda slot, part: twin_copy(slot, part).start(),
        open_norm,
        lambda slot: None,
    )

    def normalize(which):
        def block(j, _):
            rows = pl.ds(pl.multiple_of(j * 32, 32), 32)
            values = normin[which, rows, :].astype(jnp.float32)
            inv = lax.rsqrt(jnp.mean(values * values, axis=1, keepdims=True) + norm_eps)
            normed[which, rows, :] = (values * inv * gain[...]).astype(jnp.bfloat16)
            return 0

        lax.fori_loop(0, group // 32, block, 0)

    def slice_copy(which, home):
        rows = pl.ds(pl.multiple_of(home * group, group), group)
        cols = pl.ds(pl.multiple_of(sibling * own_feats, 128), own_feats)
        return send(
            normed.at[which, :, cols],
            slices.at[rows, :],
            slice_send.at[which],
            slice_recv.at[which],
            me,
            sibling,
        )

    def folded(values, join):
        result = values[:, :128]
        for at in range(128, TILE, 128):
            result = join(result, values[:, at : at + 128])
        return result

    def score(which, first, last):
        def block(j, _):
            cols = pl.ds(pl.multiple_of(j * TILE, TILE), TILE)
            values = (
                jnp.dot(normed[which], words[:, cols], preferred_element_type=jnp.float32)
                + bias[:, cols]
            )
            scores[which, :, cols] = values
            tops[which] = jnp.maximum(tops[which], folded(values, jnp.maximum))
            return 0

        lax.fori_loop(first, last, block, 0)

    def level(which):
        top = jnp.max(tops[which], axis=1, keepdims=True)
        tops[which] = jnp.broadcast_to(top, (group, 128))
        lanes[...] = jnp.zeros_like(lanes)

        def powers(j, _):
            cols = pl.ds(pl.multiple_of(j * TILE, TILE), TILE)
            values = scores[which, :, cols]
            if which == 0:
                ids = lax.broadcasted_iota(jnp.int32, (group, TILE), 1) + (me * ncols + j * TILE)
                hits = jnp.where(ids == own_goals, values, 0.0)
                lanes[1] += folded(hits, jnp.add)
            values = jnp.exp(values - top)
            scores[which, :, cols] = values
            if which == 0:
                lanes[0] += folded(values, jnp.add)
            return 0

        lax.fori_loop(0, ncols // TILE, powers, 0)
        return top

    def stat_copy(away, j, home):
        peer = lax.rem(me + j, n)
        return send(
            stats.at[0, me],
            stats.at[away, me],
            stat_send.at[away],
            stat_recv.at[away],
            peer,
            home,
        )

    own_goals = goals[:, 0:1].astype(jnp.int32)
    blocks = ncols // TILE
    normalize(0)
    load.wait()
    slice_copy(0, dp).start()
    score(0, 0, blocks)
    top = level(0)
    lane = lax.broadcasted_iota(jnp.int32, (group, 128), 1)
    packed = jnp.where(
        lane == 0,
        top,
        jnp.where(
            lane == 1,
            jnp.sum(lanes[0], axis=1, keepdims=True),
            jnp.where(
                lane == 2,
                jnp.sum(lanes[1], axis=1, keepdims=True),
                jnp.where(lane == 3, goals[...], 0.0),
            ),
        ),
    )
    stats[0, me] = jnp.transpose(packed)[:8, :]

    def start_stats(j, _):
        stat_copy(0, j, dp).start()
        return 0

    def start_away(j, _):
        stat_copy(1, j, twin).start()
        return 0

    lax.fori_loop(1, n, start_stats, 0)
    lax.fori_loop(0, n, start_away, 0)

    def wait_stats(away):
        arrived = stats.at[away, pl.ds(0, n - 1 + away)]
        await_bytes(arrived, stat_recv.at[away])
        await_bytes(arrived, stat_send.at[away])

    def score_copy(which, home, j):
        rows = pl.ds(pl.multiple_of(home * group, group), group)
        cols = pl.ds(pl.multiple_of(j * TILE, TILE), TILE)
        return send(
            dscore.at[which, :, cols],
            score_out.at[rows, cols],
            score_send.at[which],
            score_recv.at[which],
            me,
            sibling,
        )

    def keep_copy(which, home, j):
        rows = pl.ds(pl.multiple_of(home * group, group), group)
        cols = pl.ds(pl.multiple_of(j * TILE, TILE), TILE)
        return pltpu.make_async_copy(
            dscore.at[which, :, cols], score_out.at[rows, cols], keep_sem.at[which]
        )

    loss_copy = pltpu.make_async_copy(loss_buf, loss_out, out_sem.at[0])
    flip_copy = pltpu.make_async_copy(flip_buf, flip_out, out_sem.at[1])
    input_copy = pltpu.make_async_copy(input_buf, input_out, out_sem.at[2])

    def derive(which, home):
        parts = stats[which]
        highest = jnp.max(parts[:, 0, :], axis=0, keepdims=True)
        total = jnp.sum(parts[:, 1, :] * jnp.exp(parts[:, 0, :] - highest), axis=0, keepdims=True)
        lse = highest + jnp.log(total)
        if which == 0:
            goal = jnp.sum(parts[:, 2, :], axis=0, keepdims=True)
            loss_buf[...] = jnp.broadcast_to(lse - goal + zloss_weight * lse * lse, (8, group))
            loss_copy.start()
        column = lax.broadcasted_iota(jnp.int32, (128, group), 0)
        turned = jnp.transpose(
            jnp.where(column == 0, lse, jnp.where(column == 1, parts[0, 3:4, :], 0.0))
        )
        lse_col = turned[:, 0:1]
        goal_col = turned[:, 1:2].astype(jnp.int32)
        factor = jnp.exp(tops[which][:, 0:1] - lse_col) * (1.0 + 2.0 * zloss_weight * lse_col)

        def block(j, _):
            cols = pl.ds(pl.multiple_of(j * TILE, TILE), TILE)
            ids = lax.broadcasted_iota(jnp.int32, (group, TILE), 1) + (me * ncols + j * TILE)
            values = scores[which, :, cols] * factor - jnp.where(ids == goal_col, 1.0, 0.0)
            dscore[which, :, cols] = values.astype(jnp.bfloat16)
            score_copy(which, home, j).start()
            keep_copy(which, home, j).start()
            return 0

        lax.fori_loop(0, ncols // TILE, block, 0)

    wait_stats(0)
    derive(0, dp)

    def cross_copy(t):
        cols = pl.ds(pl.multiple_of(t * TILE, TILE), TILE)
        return send(
            terms.at[:, 1 - side, :, cols],
            crossing.at[:, :, cols],
            cross_send,
            cross_recv.at[t],
            other,
            dp,
        )

    def term_copy(t, j):
        peer = lax.rem(place + j, line)
        cols = pl.ds(pl.multiple_of(t * TILE, TILE), TILE)
        return send(
            sums.at[peer, :, cols],
            landed.at[place, :, cols],
            term_send,
            term_recv,
            2 * peer + side,
            dp,
        )

    def term_block(t, _):
        cols = pl.ds(pl.multiple_of(t * TILE, TILE), TILE)
        block = lax.dot_general(
            dscore[0],
            words[cols, :],
            (((1,), (1,)), ((), ())),
            preferred_element_type=jnp.float32,
        ).astype(jnp.bfloat16)
        terms[:, :, :, cols] = block.reshape(line, 2, rows_dev, TILE)
        cross_copy(t).start()
        return 0

    def pass_on(t):
        cols = pl.ds(t * TILE, TILE)
        cross_copy(t).wait_recv()
        both = terms[:, side, :, cols].astype(jnp.float32) + crossing[:, :, cols].astype(jnp.float32)
        sums[:, :, cols] = both.astype(jnp.bfloat16)
        for j in range(1, line):
            term_copy(t, j).start()
        landed[place, :, cols] = sums[place, :, cols]

    lax.fori_loop(0, width // TILE, term_block, 0)
    await_bytes(normin.at[1], twin_recv)
    await_bytes(normin.at[1], twin_send)
    normalize(1)
    slice_copy(1, twin).start()
    tiles = width // TILE
    done = 0
    for t in range(tiles):
        pass_on(t)
        if t < tiles - 1:
            upto = blocks * (t + 1) // (tiles - 1)
            score(1, done, upto)
            done = upto
    for which, home in ((0, dp), (1, twin)):
        rows = pl.ds(pl.multiple_of(home * group, group), group)
        slices[rows, :] = normed[which, :, pl.ds(pl.multiple_of(dp * own_feats, 128), own_feats)]
        slice_copy(which, home).wait()
    flip_buf[...] = jnp.transpose(slices[...])
    flip_copy.start()
    level(1)
    wait_stats(1)
    derive(1, twin)

    passed = landed.at[pl.ds(0, line - 1)]
    await_bytes(passed, term_recv)
    await_bytes(passed, term_send)
    await_bytes(crossing, cross_send)
    my_rows = pl.ds(pl.multiple_of(me * rows_dev, rows_dev), rows_dev)
    values = normin[0, my_rows, :].astype(jnp.float32)
    inv = lax.rsqrt(jnp.mean(values * values, axis=1, keepdims=True) + norm_eps)
    dnormed = landed[0].astype(jnp.float32)
    for slot in range(1, line):
        dnormed += landed[slot].astype(jnp.float32)
    scaled = dnormed * gain[...]
    input_buf[...] = inv * (
        scaled - values * inv * inv * jnp.mean(values * scaled, axis=1, keepdims=True)
    )
    input_copy.start()
    for which in range(2):
        await_bytes(dscore.at[which], keep_sem.at[which])
        await_bytes(dscore.at[which], score_send.at[which])
        await_bytes(dscore.at[which], score_recv.at[which])
    finish_units()
    finish_norm()
    loss_copy.wait()
    flip_copy.wait()
    input_copy.wait()


def vocab_kernel(
    flipped_in,
    dscore_in,
    grad_input,
    losses_in,
    vocab_out,
    input_out,
    loss_out,
    flipped,
    dscore,
    results,
    inputs,
    losses,
    loss_row,
    load_sem,
    block_sem,
    out_sem,
    tail_sem,
):
    rows_dev = loss_row.shape[1]
    group = losses.shape[1]
    count = dscore.shape[0]

    def block_in(j):
        cols = pl.ds(pl.multiple_of(j * BLOCK, BLOCK), BLOCK)
        return pltpu.make_async_copy(dscore_in.at[:, cols], dscore.at[j], block_sem.at[j])

    def block_out(j):
        cols = pl.ds(pl.multiple_of(j * BLOCK, BLOCK), BLOCK)
        return pltpu.make_async_copy(results.at[j], vocab_out.at[:, cols], out_sem.at[j])

    bring = pltpu.make_async_copy(flipped_in, flipped, load_sem.at[0])
    bring_input = pltpu.make_async_copy(grad_input, inputs, load_sem.at[1])
    bring_losses = pltpu.make_async_copy(losses_in, losses, load_sem.at[2])
    put_input = pltpu.make_async_copy(inputs, input_out, tail_sem.at[0])
    put_losses = pltpu.make_async_copy(loss_row, loss_out, tail_sem.at[1])
    bring.start()

    def start_block(j, _):
        block_in(j).start()
        return 0

    lax.fori_loop(0, count, start_block, 0)
    bring_input.start()
    bring_losses.start()
    bring.wait()

    def multiply(j, _):
        block_in(j).wait()
        results[j] = jnp.dot(flipped[...], dscore[j], preferred_element_type=jnp.float32)
        block_out(j).start()
        return 0

    def finish(j, _):
        block_out(j).wait()
        return 0

    lax.fori_loop(0, count // 2, multiply, 0)
    bring_input.wait()
    put_input.start()
    bring_losses.wait()
    shift = lax.rem(group - lax.axis_index("vp") * rows_dev, group)
    loss_row[...] = pltpu.roll(losses[...], shift, 1)[0:1, :rows_dev]
    put_losses.start()
    lax.fori_loop(count // 2, count, multiply, 0)
    put_input.wait()
    put_losses.wait()
    lax.fori_loop(0, count, finish, 0)


def fused(stream, hidden, w_down, final_gain, vocab, vocab_bias, targets):
    n = lax.axis_size("vp")
    groups = lax.axis_size("dp")
    rows_dev, width = stream.shape
    group, depth = hidden.shape
    feats = w_down.shape[1]
    ncols = vocab.shape[1]
    own_feats = width // groups
    tokens = groups * group
    line = n // 2
    f32, bf16 = jnp.float32, jnp.bfloat16
    dma = pltpu.SemaphoreType.DMA
    hbm = pl.BlockSpec(memory_space=pl.ANY)
    group_losses, grad_input, dscore, flipped = pl.pallas_call(
        functools.partial(head_kernel, n),
        out_shape=(
            jax.ShapeDtypeStruct((8, group), f32),
            jax.ShapeDtypeStruct((rows_dev, width), f32),
            jax.ShapeDtypeStruct((tokens, ncols), bf16),
            jax.ShapeDtypeStruct((own_feats, tokens), bf16),
        ),
        in_specs=[hbm] * 7,
        out_specs=(hbm,) * 4,
        scratch_shapes=[
            pltpu.VMEM(w_down.shape, bf16),
            pltpu.VMEM((rows_dev, width), bf16),
            pltpu.VMEM((1, width), f32),
            pltpu.VMEM((1, ncols), f32),
            pltpu.VMEM((1, group), jnp.int32),
            pltpu.VMEM((8, group), f32),
            pltpu.VMEM((rows_dev, width), f32),
            pltpu.VMEM((own_feats, tokens), bf16),
            pltpu.VMEM((n * depth, group), bf16),
            pltpu.VMEM((group, feats), bf16),
            pltpu.VMEM((2, group, width), bf16),
            pltpu.VMEM((2, group, width), bf16),
            pltpu.VMEM((width, ncols), bf16),
            pltpu.VMEM((2, group, ncols), f32),
            pltpu.VMEM((2, group, 128), f32),
            pltpu.VMEM((2, group, 128), f32),
            pltpu.VMEM((2, n, 8, group), f32),
            pltpu.VMEM((group, 128), f32),
            pltpu.VMEM((group, feats), f32),
            pltpu.VMEM((2, group, ncols), bf16),
            pltpu.VMEM((tokens, own_feats), bf16),
            pltpu.VMEM((line, 2, rows_dev, width), bf16),
            pltpu.VMEM((line, rows_dev, width), bf16),
            pltpu.VMEM((line, rows_dev, width), bf16),
            pltpu.VMEM((line, rows_dev, width), bf16),
            dma((3,)),
            dma((n, UNIT_PARTS)),
            dma((3,)),
            dma((n, NORM_PARTS)),
            dma,
            dma,
            dma,
            dma,
            dma((2,)),
            dma((2,)),
            dma((2,)),
            dma((2,)),
            dma((2,)),
            dma((2,)),
            dma,
            dma((width // TILE,)),
            dma,
            dma,
            dma((7,)),
            dma((2,)),
            dma((3,)),
        ],
        compiler_params=pltpu.CompilerParams(
            collective_id=0, has_side_effects=True, vmem_limit_bytes=64 * 1024 * 1024 - 65536
        ),
    )(
        hidden.T,
        w_down,
        stream,
        final_gain.reshape(1, width),
        vocab,
        vocab_bias.reshape(1, ncols),
        targets.reshape(1, group),
    )

    count = ncols // BLOCK
    grad_vocab, grad_input, losses = pl.pallas_call(
        vocab_kernel,
        out_shape=(
            jax.ShapeDtypeStruct((own_feats, ncols), f32),
            jax.ShapeDtypeStruct((rows_dev, width), f32),
            jax.ShapeDtypeStruct((1, rows_dev), f32),
        ),
        in_specs=[hbm] * 4,
        out_specs=(hbm,) * 3,
        scratch_shapes=[
            pltpu.VMEM((own_feats, tokens), bf16),
            pltpu.VMEM((count, tokens, BLOCK), bf16),
            pltpu.VMEM((count, own_feats, BLOCK), f32),
            pltpu.VMEM((rows_dev, width), f32),
            pltpu.VMEM((8, group), f32),
            pltpu.VMEM((1, rows_dev), f32),
            dma((3,)),
            dma((count,)),
            dma((count,)),
            dma((2,)),
        ],
        compiler_params=pltpu.CompilerParams(vmem_limit_bytes=64 * 1024 * 1024 - 65536),
    )(flipped, dscore, grad_input, group_losses)
    return (losses.reshape(rows_dev), grad_input, grad_vocab)


def choose(stream, hidden, w_down, final_gain, vocab, vocab_bias, targets):
    rows_dev, width = stream.shape
    group, depth = hidden.shape
    n, groups = lax.axis_size("vp"), lax.axis_size("dp")
    tiles = (
        n % 2 == 0
        and groups == 4
        and rows_dev % 32 == 0
        and depth % (16 * UNIT_PARTS) == 0
        and group % (32 * NORM_PARTS) == 0
        and w_down.shape[1] % 128 == 0
        and width % TILE == 0
        and (width // groups) % 128 == 0
        and vocab.shape[1] % TILE == 0
    )
    path = fused if tiles else body
    return path(stream, hidden, w_down, final_gain, vocab, vocab_bias, targets)


def solution(mesh):
    placed = (
        P(("dp", "vp"), None),
        P("dp", "vp"),
        P(None, "vp"),
        P(),
        P(None, "vp"),
        P("vp"),
        P("dp"),
    )
    return jax.shard_map(
        choose,
        mesh=mesh,
        in_specs=placed,
        out_specs=(P(("dp", "vp")), P(("dp", "vp"), None), P("dp", "vp")),
        check_vma=False,
    )
```

```python
import functools

import jax
import jax.numpy as jnp
from jax import lax
from jax.experimental import pallas as pl
from jax.experimental.pallas import tpu as pltpu
from jax.sharding import PartitionSpec as P

norm_eps = 1e-06
zloss_weight = 0.001


def combined_all(value, axis, join):
    pieces = jax.tree.map(lambda part: lax.all_gather(part, axis), value)
    head = jax.tree.map(lambda part: part[0], pieces)
    tail = jax.tree.map(lambda part: part[1:], pieces)
    total, _ = lax.scan(lambda total, section: (join(total, section), None), head, tail)
    return total


def combine_stats(first, second):
    top = jnp.maximum(first[0], second[0])
    total = first[1] * jnp.exp(first[0] - top) + second[1] * jnp.exp(second[0] - top)
    return (top, total, first[2] + second[2])


def body(stream, hidden, w_down, final_gain, vocab, vocab_bias, targets):
    rows_dev = stream.shape[0]
    width = stream.shape[1]
    group = targets.shape[0]
    mine = lax.axis_index("vp")
    feat_cols = w_down.shape[1]
    proj = jnp.dot(
        lax.all_gather(hidden, "vp", axis=1, tiled=True), w_down, preferred_element_type=jnp.float32
    )
    stream_cols = lax.all_to_all(stream, "vp", split_axis=1, concat_axis=0, tiled=True)
    normin_cols = (stream_cols.astype(jnp.float32) + proj).astype(jnp.bfloat16)
    col_values = normin_cols.astype(jnp.float32)
    square_total = lax.psum(jnp.sum(col_values * col_values, axis=1), "vp")
    inv_group = lax.rsqrt(square_total / width + norm_eps)
    gain_cols = lax.dynamic_slice_in_dim(final_gain, mine * feat_cols, feat_cols)
    normed_cols = (col_values * inv_group[:, None] * gain_cols).astype(jnp.bfloat16)
    normed = lax.all_gather(normed_cols, "vp", axis=1, tiled=True)
    normin = lax.all_to_all(normin_cols, "vp", split_axis=0, concat_axis=1, tiled=True)
    values = normin.astype(jnp.float32)
    inv = lax.rsqrt(jnp.mean(values * values, axis=1, keepdims=True) + norm_eps)
    ncols = vocab.shape[1]
    scores = jnp.dot(normed, vocab, preferred_element_type=jnp.float32) + vocab_bias
    local_top = jnp.max(scores, axis=1)
    local_total = jnp.sum(jnp.exp(scores - local_top[:, None]), axis=1)
    column_ids = lax.broadcasted_iota(jnp.int32, (group, ncols), 1) + mine * ncols
    hit = column_ids == targets[:, None]
    local_target = jnp.sum(jnp.where(hit, scores, 0.0), axis=1)
    top, total, target_score = combined_all(
        (local_top, local_total, local_target), "vp", combine_stats
    )
    lse = top + jnp.log(total)
    group_losses = lse - target_score + zloss_weight * lse * lse
    losses = lax.dynamic_slice_in_dim(group_losses, mine * rows_dev, rows_dev)
    probs = jnp.exp(scores - lse[:, None])
    dscore = (probs * (1.0 + 2.0 * zloss_weight * lse)[:, None] - jnp.where(hit, 1.0, 0.0)).astype(
        jnp.bfloat16
    )
    feat_group = width // lax.axis_size("dp")
    feat_start = lax.axis_index("dp") * feat_group
    rows_slice = lax.dynamic_slice_in_dim(
        lax.all_gather(normed, "dp", axis=0, tiled=True), feat_start, feat_group, 1
    )
    grad_vocab = lax.dot_general(
        rows_slice,
        lax.all_gather(dscore, "dp", axis=0, tiled=True),
        (((0,), (0,)), ((), ())),
        preferred_element_type=jnp.float32,
    )
    row_term = lax.dot_general(
        dscore, vocab, (((1,), (1,)), ((), ())), preferred_element_type=jnp.float32
    )
    row_parts = lax.all_to_all(
        row_term[:, None, :].astype(jnp.bfloat16), "vp", split_axis=0, concat_axis=1, tiled=True
    ).astype(jnp.float32)
    dnormed = jnp.sum(row_parts, axis=1)
    scaled = dnormed * final_gain
    grad_input = inv * (
        scaled - values * inv * inv * jnp.mean(values * scaled, axis=1, keepdims=True)
    )
    return (losses, grad_input, grad_vocab)


MESH = pl.DeviceIdType.MESH
UNIT_PARTS = 2
NORM_PARTS = 4
TILE = 512
BLOCK = 512
AHEAD = 4


def send(src, dst, send_sem, recv_sem, vp, dp):
    return pltpu.make_async_remote_copy(
        src_ref=src,
        dst_ref=dst,
        send_sem=send_sem,
        recv_sem=recv_sem,
        device_id={"vp": vp, "dp": dp},
        device_id_type=MESH,
    )


def gather(n, me, dp, parts, own, place, bulk, sems, extra, first, use):
    line = n // 2
    here = me // 2
    side = me - 2 * here
    other = me + 1 - 2 * side
    turn = parts // 2
    send_sem, recv_sem = sems
    targets = {0: other, 1: me + 2, 2: me - 2}
    sent = []

    def copy(way, slot, part, src=None):
        return send(
            place(slot, part) if src is None else src,
            place(slot, part),
            send_sem.at[way],
            recv_sem.at[slot, part],
            targets[way],
            dp,
        )

    def holds(conditions, row):
        return functools.reduce(lambda a, b: a & b, [test(row) for test in conditions])

    def when(conditions, action):
        if conditions:
            pl.when(holds(conditions, here))(action)
        else:
            action()

    def put(outer, inner, way, slot, part, src=None):
        when(inner, lambda: copy(way, slot, part, src).start())
        sent.append((outer + inner, way))

    def live(step):
        if step == 0:
            return []
        return [lambda row: (row + step < line) & (row + step >= 0)]

    def ends(step):
        return [lambda row: row + step == (line - 1 if step > 0 else 0)]

    def inside(step):
        return [lambda row: row + step != (line - 1 if step > 0 else 0)]

    up, down = [lambda row: row < line - 1], [lambda row: row > 0]

    for part in range(parts):
        put([], [], 0, me, part, own(part))
        put([], up, 1, me, part, own(part))
        put([], down, 2, me, part, own(part))
        extra(me, part)
    first()

    def straight(k, part, step, way):
        slot = me + 2 * step
        outer = live(step)

        def receive():
            copy(0, slot, part).wait_recv()
            put(outer, up if way == 1 else down, way, slot, part)
            put(outer, inside(step) if part >= turn else [], 0, slot, part)
            extra(slot, part)

        when(outer, receive)

    def routed(k):
        for step, way in ((-k, 1), (k, 2)):
            slot = other + 2 * step
            outer = live(step) + ends(step)

            def receive(slot=slot, outer=outer, way=way):
                for part in range(turn, parts):
                    copy(0, slot, part).wait_recv()
                    put(outer, up if way == 1 else down, way, slot, part)
                    extra(slot, part)

            when(outer, receive)

    def crossed(k):
        for part in range(parts):
            for step in (-k, k) if k else (0,):
                slot = other + 2 * step
                outer = live(step)
                if k and part >= turn:
                    outer = outer + inside(step)

                def receive(slot=slot, part=part):
                    copy(0, slot, part).wait_recv()
                    extra(slot, part)

                when(outer, receive)
                if k == 0 and part >= turn:
                    put([], [lambda row: row == 0] + up, 1, slot, part)
                    put([], [lambda row: row == line - 1] + down, 2, slot, part)

    def used(base, k):
        for step in (-k, k) if k else (0,):
            when(live(step), lambda step=step: use(base + 2 * step))

    for k in range(1, line):
        for part in range(parts):
            straight(k, part, -k, 1)
            straight(k, part, k, 2)
        if k > 1:
            routed(k - 1)
        crossed(k - 1)
        used(me, k)
        used(other, k - 1)
    if line > 1:
        routed(line - 1)
    crossed(line - 1)
    used(other, line - 1)

    def finish():
        for way in range(3):
            for row in range(line):
                count = sum(1 for tests, which in sent if which == way and (not tests or holds(tests, row)))
                if count:
                    pl.when(here == row)(lambda: await_bytes(bulk(count), send_sem.at[way]))

    return finish


def await_bytes(ref, sem):
    pltpu.make_async_copy(ref, ref, sem).wait()


def head_kernel(
    n,
    hidden,
    w_down_in,
    stream_in,
    gain_in,
    vocab,
    bias_in,
    targets_in,
    loss_out,
    landed,
    score_out,
    flip_out,
    rows_out,
    w_down,
    stream,
    gain,
    bias,
    targets,
    loss_buf,
    flip_buf,
    units,
    stream_cols,
    normin,
    normed,
    words,
    scores,
    squared,
    lanes,
    lines,
    goal_ids,
    raw,
    stage,
    stats,
    goals,
    total,
    dscore,
    slices,
    terms,
    crossing,
    sums,
    unit_send,
    unit_recv,
    norm_send,
    norm_recv,
    stream_send,
    stream_recv,
    twin_send,
    twin_recv,
    stat_send,
    stat_recv,
    score_send,
    score_recv,
    slice_send,
    slice_recv,
    cross_send,
    cross_recv,
    term_send,
    term_recv,
    load_sem,
    keep_sem,
    out_sem,
    twin_ready,
):
    me = lax.axis_index("vp")
    dp = lax.axis_index("dp")
    twin = lax.rem(dp + 2, 4)
    core = lax.rem(dp, 2)
    sibling = dp + 1 - 2 * core
    line = n // 2
    place = me // 2
    side = me - 2 * place
    other = me + 1 - 2 * side
    depth, group = hidden.shape
    width = gain.shape[1]
    feats = stream_cols.shape[1]
    rows_dev = stream.shape[0]
    ncols = bias.shape[1]
    own_feats = slices.shape[1]
    half = group // NORM_PARTS
    piece = depth // UNIT_PARTS

    barrier = pltpu.get_barrier_semaphore()

    above, below = place < line - 1, place > 0

    def greet(vp, home):
        pl.semaphore_signal(barrier, 1, device_id={"vp": vp, "dp": home}, device_id_type=MESH)

    greet(me, twin)
    greet(me, sibling)
    greet(other, dp)
    pl.when(above)(lambda: greet(me + 2, dp))
    pl.when(below)(lambda: greet(me - 2, dp))

    def brought(at, src, dst):
        return pltpu.make_async_copy(src, dst, load_sem.at[at])

    bring = brought(0, hidden, units.at[pl.ds(pl.multiple_of(me * depth, 16), depth), :])
    bring_stream = brought(1, stream_in, stream)
    bring_down = brought(2, w_down_in, w_down)
    bring_targets = brought(3, targets_in, targets)
    bring_gain = brought(4, gain_in, gain)
    bring_bias = brought(5, bias_in, bias)
    load = brought(6, vocab, words)
    for copy in (bring, bring_stream, bring_down, bring_targets, bring_gain, bring_bias, load):
        copy.start()
    pl.semaphore_wait(barrier, 3 + above.astype(jnp.int32) + below.astype(jnp.int32))

    def stream_copy(peer):
        return send(
            stream.at[:, pl.ds(pl.multiple_of(peer * feats, 128), feats)],
            stream_cols.at[pl.ds(pl.multiple_of(me * rows_dev, rows_dev), rows_dev), :],
            stream_send,
            stream_recv,
            peer,
            dp,
        )

    def pair_streams(slot, part):
        if part == 0:
            pl.when((lax.rem(slot, 2) == side) & (slot != me))(lambda: pair_stream(slot))

    def pair_stream(slot):
        stream_copy(slot).start()
        stream_copy(slot + 1 - 2 * side).start()

    def place_units(slot, part):
        return units.at[pl.ds(pl.multiple_of(slot * depth + part * piece, 16), piece), :]

    def product(slot):
        rows = pl.ds(pl.multiple_of(slot * depth, 16), depth)
        return lax.dot_general(
            units[rows, :],
            w_down[rows, :],
            (((0,), (0,)), ((), ())),
            preferred_element_type=jnp.float32,
        )

    def open_units():
        bring_stream.wait()
        stream_copy(other).start()
        stream_cols[pl.ds(pl.multiple_of(me * rows_dev, rows_dev), rows_dev), :] = stream[
            :, pl.ds(pl.multiple_of(me * feats, 128), feats)
        ]
        bring_targets.wait()
        goals[...] = jnp.transpose(
            jnp.broadcast_to(targets[...].astype(jnp.float32), (128, group))
        )
        goal_ids[0] = goals[...].astype(jnp.int32)
        bring_down.wait()
        total[...] = product(me)

    def project(slot):
        total[...] += product(slot)

    bring.wait()
    finish_units = gather(
        n,
        me,
        dp,
        UNIT_PARTS,
        lambda part: place_units(me, part),
        place_units,
        lambda count: units.at[pl.ds(0, count * piece), :],
        (unit_send, unit_recv),
        pair_streams,
        open_units,
        project,
    )
    streamed = stream_cols.at[pl.ds(0, (n - 1) * rows_dev), :]
    await_bytes(streamed, stream_recv)
    await_bytes(streamed, stream_send)

    pl.semaphore_signal(twin_ready, 1, device_id={"vp": me, "dp": twin}, device_id_type=MESH)

    def cols_of(slot):
        return pl.ds(pl.multiple_of(slot * feats, 128), feats)

    normin[0, :, cols_of(me)] = (stream_cols[...].astype(jnp.float32) + total[...]).astype(jnp.bfloat16)

    def twin_copy(slot, part):
        rows = pl.ds(part * half, half)
        return send(
            normin.at[0, rows, cols_of(slot)],
            normin.at[1, rows, cols_of(slot)],
            twin_send,
            twin_recv,
            me,
            twin,
        )

    def place_norm(slot, part):
        return normin.at[0, pl.ds(part * half, half), cols_of(slot)]

    def folded(pieces, join):
        return functools.reduce(join, pieces)

    def add_squares(slot):
        values = normin[0, :, cols_of(slot)].astype(jnp.float32)
        squares = values * values
        squared[...] += folded([squares[:, at : at + 128] for at in range(0, feats, 128)], jnp.add)

    def open_norm():
        squared[...] = jnp.zeros_like(squared)
        add_squares(me)
        bring_gain.wait()
        bring_bias.wait()
        lanes[0] = jnp.full((group, 128), -jnp.inf, jnp.float32)
        lanes[1] = jnp.zeros((group, 128), jnp.float32)
        lanes[2] = jnp.zeros((group, 128), jnp.float32)

    finish_norm = gather(
        n,
        me,
        dp,
        NORM_PARTS,
        lambda part: place_norm(me, part),
        place_norm,
        lambda count: scores.at[pl.ds(0, count * half // 8), pl.ds(0, 4 * feats)],
        (norm_send, norm_recv),
        lambda slot, part: twin_copy(slot, part).start(),
        open_norm,
        add_squares,
    )

    def normalize(which):
        if which == 0:
            mean = jnp.sum(squared[...], axis=1, keepdims=True) / width
            squared[...] = jnp.broadcast_to(lax.rsqrt(mean + norm_eps), (group, 128))

        def block(j, _):
            rows = pl.ds(pl.multiple_of(j * 32, 32), 32)
            values = normin[which, rows, :].astype(jnp.float32)
            if which == 0:
                inv = squared[rows, 0:1]
            else:
                inv = lax.rsqrt(jnp.mean(values * values, axis=1, keepdims=True) + norm_eps)
            normed[which, rows, :] = (values * inv * gain[...]).astype(jnp.bfloat16)
            return 0

        lax.fori_loop(0, group // 32, block, 0)

    def slice_copy(which, home):
        rows = pl.ds(pl.multiple_of(home * group, group), group)
        cols = pl.ds(pl.multiple_of(sibling * own_feats, 128), own_feats)
        return send(
            normed.at[which, :, cols],
            slices.at[rows, :],
            slice_send.at[which],
            slice_recv.at[which],
            me,
            sibling,
        )

    def is_goal(j, at, goal):
        ids = lax.broadcasted_iota(jnp.int32, (group, 128), 1) + (me * ncols + j * TILE + at)
        return ids == goal

    def block_cols(j):
        return pl.ds(pl.multiple_of(j * TILE, TILE), TILE)

    def piece_cols(j, i):
        return pl.ds(pl.multiple_of(j * TILE + i * 128, 128), 128)

    def multiply(which, j, slot):
        raw[slot] = jnp.dot(
            normed[which], words[:, block_cols(j)], preferred_element_type=jnp.float32
        )

    def raw_pieces(j, slot):
        return [
            raw[slot, :, at : at + 128] + bias[:, piece_cols(j, at // 128)]
            for at in range(0, TILE, 128)
        ]

    def pairs(which, absorb, first, last, after=None):
        def body(i, _):
            multiply(which, 2 * i + 1, 1)
            absorb(2 * i, 0)
            multiply(which, 2 * i + 2, 0)
            absorb(2 * i + 1, 1)
            if after:
                after(i)
            return 0

        final = last == blocks // 2
        lax.fori_loop(first, last - 1 if final else last, body, 0)
        if final:
            multiply(which, blocks - 1, 1)
            absorb(blocks - 2, 0)
            absorb(blocks - 1, 1)
            if after:
                after(last - 1)

    def absorb_own(j, slot):
        pieces = raw_pieces(j, slot)
        before = lanes[0]
        peak = jnp.maximum(before, folded(pieces, jnp.maximum))
        powers = [jnp.exp(piece - peak) for piece in pieces]
        for i, piece in enumerate(pieces):
            scores[:, piece_cols(j, i)] = piece
        lanes[0] = peak
        lanes[1] = lanes[1] * jnp.exp(before - peak) + folded(powers, jnp.add)
        hits = [
            jnp.where(is_goal(j, 128 * i, goal_ids[0]), piece, 0.0) for i, piece in enumerate(pieces)
        ]
        lanes[2] += folded(hits, jnp.add)

    def stat_copy(away, j, home):
        peer = lax.rem(me + j, n)
        return send(
            stats.at[0, me],
            stats.at[away, me],
            stat_send.at[away],
            stat_recv.at[away],
            peer,
            home,
        )

    blocks = ncols // TILE
    normalize(0)
    load.wait()
    slice_copy(0, dp).start()
    multiply(0, 0, 0)
    pairs(0, absorb_own, 0, blocks // 2)
    top = jnp.max(lanes[0], axis=1, keepdims=True)
    weight = jnp.sum(lanes[1] * jnp.exp(lanes[0] - top), axis=1, keepdims=True)
    lane = lax.broadcasted_iota(jnp.int32, (group, 128), 1)
    packed = jnp.where(
        lane == 0,
        top,
        jnp.where(
            lane == 1,
            weight,
            jnp.where(
                lane == 2,
                jnp.sum(lanes[2], axis=1, keepdims=True),
                jnp.where(lane == 3, goals[...], 0.0),
            ),
        ),
    )
    stats[0, me] = jnp.transpose(packed)[:8, :]

    def start_stats(j, _):
        stat_copy(0, j, dp).start()
        return 0

    def start_away(j, _):
        stat_copy(1, j, twin).start()
        return 0

    lax.fori_loop(1, n, start_stats, 0)
    pl.semaphore_wait(twin_ready, 1)
    lax.fori_loop(0, n, start_away, 0)

    def wait_stats(away):
        arrived = stats.at[away, pl.ds(0, n - 1 + away)]
        await_bytes(arrived, stat_recv.at[away])
        await_bytes(arrived, stat_send.at[away])

    def pair_cols(i):
        return pl.ds(pl.multiple_of(i * 2 * TILE, 2 * TILE), 2 * TILE)

    def score_copy(which, home, j):
        rows = pl.ds(pl.multiple_of(home * group, group), group)
        cols = pair_cols(j)
        return send(
            dscore.at[which, :, cols],
            score_out.at[rows, cols],
            score_send.at[which],
            score_recv.at[which],
            me,
            sibling,
        )

    def keep_copy(which, home, j):
        rows = pl.ds(pl.multiple_of(home * group, group), group)
        cols = pair_cols(j)
        return pltpu.make_async_copy(
            dscore.at[which, :, cols], score_out.at[rows, cols], keep_sem.at[which]
        )

    loss_copy = pltpu.make_async_copy(loss_buf, loss_out, out_sem.at[0])
    flip_copy = pltpu.make_async_copy(flip_buf, flip_out, out_sem.at[1])
    rows_copy = pltpu.make_async_copy(
        normin.at[0, pl.ds(pl.multiple_of(me * rows_dev, rows_dev), rows_dev), :],
        rows_out,
        out_sem.at[2],
    )

    def send_scores(which, home, j):
        score_copy(which, home, j).start()
        keep_copy(which, home, j).start()

    def summary(which):
        parts = stats[which]
        highest = jnp.max(parts[:, 0, :], axis=0, keepdims=True)
        total = jnp.sum(parts[:, 1, :] * jnp.exp(parts[:, 0, :] - highest), axis=0, keepdims=True)
        lse = highest + jnp.log(total)
        if which == 0:
            goal = jnp.sum(parts[:, 2, :], axis=0, keepdims=True)
            loss_buf[...] = jnp.broadcast_to(lse - goal + zloss_weight * lse * lse, (8, group))
            loss_copy.start()
        column = lax.broadcasted_iota(jnp.int32, (128, group), 0)
        turned = jnp.transpose(
            jnp.where(column == 0, lse, jnp.where(column == 1, parts[0, 3:4, :], 0.0))
        )
        lse_col = turned[:, 0:1]
        return lse_col, 1.0 + 2.0 * zloss_weight * lse_col, turned[:, 1:2].astype(jnp.int32)

    def spread(which):
        lse, slope, goal = summary(which)
        lines[0] = jnp.broadcast_to(lse, (group, 128))
        lines[1] = jnp.broadcast_to(slope, (group, 128))
        goal_ids[which] = jnp.broadcast_to(goal, (group, 128))

    def derive_own():
        spread(0)

        def derive(j, slot):
            lse, slope, goal = lines[0], lines[1], goal_ids[0]
            for i in range(TILE // 128):
                hit = jnp.where(is_goal(j, 128 * i, goal), 1.0, 0.0)
                power = jnp.exp(scores[:, piece_cols(j, i)] - lse)
                values = (power * slope - hit).astype(jnp.bfloat16)
                dscore[0, :, piece_cols(j, i)] = values
                stage[slot, :, i * 128 : (i + 1) * 128] = values

        def accumulate(j, slot):
            raw[0] += lax.dot_general(
                stage[slot],
                words[pl.ds(0, TILE), block_cols(j)],
                (((1,), (1,)), ((), ())),
                preferred_element_type=jnp.float32,
            )

        def body(i, _):
            derive(2 * i + 1, 1)
            accumulate(2 * i, 0)
            derive(2 * i + 2, 0)
            accumulate(2 * i + 1, 1)
            return 0

        raw[0] = jnp.zeros((group, TILE), jnp.float32)
        derive(0, 0)
        lax.fori_loop(0, blocks // 2 - 1, body, 0)
        derive(blocks - 1, 1)
        accumulate(blocks - 2, 0)
        accumulate(blocks - 1, 1)
        put_terms(0, raw[0])

    def absorb_twin(j, slot):
        lse, slope, goal = lines[0], lines[1], goal_ids[1]
        for i, piece in enumerate(raw_pieces(j, slot)):
            hit = jnp.where(is_goal(j, 128 * i, goal), 1.0, 0.0)
            values = jnp.exp(piece - lse) * slope - hit
            dscore[1, :, piece_cols(j, i)] = values.astype(jnp.bfloat16)


    def cross_copy(t):
        cols = pl.ds(pl.multiple_of(t * TILE, TILE), TILE)
        return send(
            terms.at[:, 1 - side, :, cols],
            crossing.at[:, :, cols],
            cross_send,
            cross_recv.at[t],
            other,
            dp,
        )

    def term_copy(t, j):
        peer = lax.rem(place + j, line)
        cols = pl.ds(pl.multiple_of(t * TILE, TILE), TILE)
        return send(
            sums.at[peer, :, cols],
            landed.at[place, :, cols],
            term_send,
            term_recv,
            2 * peer + side,
            dp,
        )

    def put_terms(t, block):
        cols = pl.ds(pl.multiple_of(t * TILE, TILE), TILE)
        terms[:, :, :, cols] = block.astype(jnp.bfloat16).reshape(line, 2, rows_dev, TILE)
        cross_copy(t).start()

    def term_block(t, _):
        cols = pl.ds(pl.multiple_of(t * TILE, TILE), TILE)
        block = lax.dot_general(
            dscore[0],
            words[cols, :],
            (((1,), (1,)), ((), ())),
            preferred_element_type=jnp.float32,
        )
        put_terms(t, block)
        return 0

    def own_copy(t):
        cols = pl.ds(pl.multiple_of(t * TILE, TILE), TILE)
        return pltpu.make_async_copy(
            sums.at[place, :, cols], landed.at[place, :, cols], out_sem.at[3]
        )

    def pass_on(t):
        cols = pl.ds(t * TILE, TILE)
        cross_copy(t).wait_recv()
        both = terms[:, side, :, cols].astype(jnp.float32) + crossing[:, :, cols].astype(jnp.float32)
        sums[:, :, cols] = both.astype(jnp.bfloat16)
        for j in range(1, line):
            term_copy(t, j).start()
        own_copy(t).start()

    rows_copy.start()
    await_bytes(normin.at[1], twin_recv)
    await_bytes(normin.at[1], twin_send)
    normalize(1)
    slice_copy(1, twin).start()
    wait_stats(0)
    derive_own()
    tiles = width // TILE
    lax.fori_loop(1, tiles, term_block, 0)
    def release(first, last):
        for i in range(blocks // 2 * first // 4, blocks // 2 * last // 4):
            send_scores(0, dp, i)

    release(0, 2)
    wait_stats(1)
    spread(1)
    multiply(1, 0, 0)

    def turn_slices():
        for which, home in ((0, dp), (1, twin)):
            rows = pl.ds(pl.multiple_of(home * group, group), group)
            own_cols = pl.ds(pl.multiple_of(dp * own_feats, 128), own_feats)
            slices[rows, :] = normed[which, :, own_cols]
            slice_copy(which, home).wait()
        flip_buf[...] = jnp.transpose(slices[...])
        flip_copy.start()

    def score_twin(first, last):
        pairs(1, absorb_twin, first, last, lambda i: send_scores(1, twin, i))

    halfway = blocks // 4
    for t in range(tiles):
        pass_on(t)
        if t < 2:
            release(2 + t, 3 + t)
        if t < tiles - 2:
            score_twin(halfway * t // (tiles - 2), halfway * (t + 1) // (tiles - 2))
        elif t == tiles - 2:
            turn_slices()
    score_twin(halfway, blocks // 2)
    passed = sums.at[pl.ds(0, line - 1)]
    await_bytes(passed, term_recv)
    await_bytes(passed, term_send)
    await_bytes(crossing, cross_send)
    await_bytes(sums.at[0], out_sem.at[3])
    for which in range(2):
        await_bytes(dscore.at[which], keep_sem.at[which])
        await_bytes(dscore.at[which], score_send.at[which])
        await_bytes(dscore.at[which], score_recv.at[which])
    finish_units()
    finish_norm()
    loss_copy.wait()
    flip_copy.wait()
    rows_copy.wait()


def vocab_kernel(
    flipped_in,
    dscore_in,
    landed_in,
    rows_in,
    gain_in,
    losses_in,
    vocab_out,
    input_out,
    loss_out,
    flipped,
    dscore,
    results,
    landed,
    rows,
    gain,
    inputs,
    losses,
    loss_row,
    load_sem,
    block_sem,
    out_sem,
    tail_sem,
):
    rows_dev = loss_row.shape[1]
    group = losses.shape[1]
    count = dscore.shape[0]

    def block_in(j):
        cols = pl.ds(pl.multiple_of(j * BLOCK, BLOCK), BLOCK)
        return pltpu.make_async_copy(dscore_in.at[:, cols], dscore.at[j], block_sem.at[j])

    def block_out(j):
        cols = pl.ds(pl.multiple_of(j * BLOCK, BLOCK), BLOCK)
        return pltpu.make_async_copy(results.at[j], vocab_out.at[:, cols], out_sem.at[j])

    loads = [
        pltpu.make_async_copy(src, dst, load_sem.at[i])
        for i, (src, dst) in enumerate(
            [
                (flipped_in, flipped),
                (landed_in, landed),
                (rows_in, rows),
                (gain_in, gain),
                (losses_in, losses),
            ]
        )
    ]
    put_input = pltpu.make_async_copy(inputs, input_out, tail_sem.at[0])
    put_losses = pltpu.make_async_copy(loss_row, loss_out, tail_sem.at[1])
    loads[0].start()
    block_in(0).start()
    for load in loads[1:]:
        load.start()
    for j in range(1, min(AHEAD, count)):
        block_in(j).start()

    def multiply(j, _):
        @pl.when(j + AHEAD - 1 < count)
        def _():
            block_in(j + AHEAD - 1).start()

        block_in(j).wait()
        results[j] = jnp.dot(flipped[...], dscore[j], preferred_element_type=jnp.float32)
        block_out(j).start()
        return 0

    for load in loads:
        load.wait()
    block_in(0).wait()
    results[0] = jnp.dot(flipped[...], dscore[0], preferred_element_type=jnp.float32)
    values = rows[...].astype(jnp.float32)
    inv = lax.rsqrt(jnp.mean(values * values, axis=1, keepdims=True) + norm_eps)
    dnormed = landed[0].astype(jnp.float32)
    for slot in range(1, landed.shape[0]):
        dnormed += landed[slot].astype(jnp.float32)
    scaled = dnormed * gain[...]
    inputs[...] = inv * (
        scaled - values * inv * inv * jnp.mean(values * scaled, axis=1, keepdims=True)
    )
    shift = lax.rem(group - lax.axis_index("vp") * rows_dev, group)
    loss_row[...] = pltpu.roll(losses[...], shift, 1)[0:1, :rows_dev]
    block_out(0).start()
    put_input.start()
    put_losses.start()

    def finish(j, _):
        block_out(j).wait()
        return 0

    lax.fori_loop(1, count, multiply, 0)
    put_input.wait()
    put_losses.wait()
    lax.fori_loop(0, count, finish, 0)


def vocab_call(flipped, dscore, landed, rows, gain, group_losses):
    own_feats, tokens = flipped.shape
    ncols = dscore.shape[1]
    line, rows_dev, width = landed.shape
    group = group_losses.shape[1]
    f32, bf16 = jnp.float32, jnp.bfloat16
    dma = pltpu.SemaphoreType.DMA
    hbm = pl.BlockSpec(memory_space=pl.ANY)
    count = ncols // BLOCK
    return pl.pallas_call(
        vocab_kernel,
        out_shape=(
            jax.ShapeDtypeStruct((own_feats, ncols), f32),
            jax.ShapeDtypeStruct((rows_dev, width), f32),
            jax.ShapeDtypeStruct((1, rows_dev), f32),
        ),
        in_specs=[hbm] * 6,
        out_specs=(hbm,) * 3,
        scratch_shapes=[
            pltpu.VMEM((own_feats, tokens), bf16),
            pltpu.VMEM((count, tokens, BLOCK), bf16),
            pltpu.VMEM((count, own_feats, BLOCK), f32),
            pltpu.VMEM((line, rows_dev, width), bf16),
            pltpu.VMEM((rows_dev, width), bf16),
            pltpu.VMEM((1, width), f32),
            pltpu.VMEM((rows_dev, width), f32),
            pltpu.VMEM((8, group), f32),
            pltpu.VMEM((1, rows_dev), f32),
            dma((5,)),
            dma((count,)),
            dma((count,)),
            dma((2,)),
        ],
        compiler_params=pltpu.CompilerParams(vmem_limit_bytes=64 * 1024 * 1024 - 65536),
    )(flipped, dscore, landed, rows, gain, group_losses)


def fused(stream, hidden, w_down, final_gain, vocab, vocab_bias, targets):
    n = lax.axis_size("vp")
    groups = lax.axis_size("dp")
    rows_dev, width = stream.shape
    group, depth = hidden.shape
    feats = w_down.shape[1]
    ncols = vocab.shape[1]
    own_feats = width // groups
    tokens = groups * group
    line = n // 2
    f32, bf16 = jnp.float32, jnp.bfloat16
    dma = pltpu.SemaphoreType.DMA
    hbm = pl.BlockSpec(memory_space=pl.ANY)
    gain = final_gain.reshape(1, width)
    group_losses, landed, dscore, flipped, rows = pl.pallas_call(
        functools.partial(head_kernel, n),
        out_shape=(
            jax.ShapeDtypeStruct((8, group), f32),
            jax.ShapeDtypeStruct((line, rows_dev, width), bf16),
            jax.ShapeDtypeStruct((tokens, ncols), bf16),
            jax.ShapeDtypeStruct((own_feats, tokens), bf16),
            jax.ShapeDtypeStruct((rows_dev, width), bf16),
        ),
        in_specs=[hbm] * 7,
        out_specs=(hbm,) * 5,
        scratch_shapes=[
            pltpu.VMEM(w_down.shape, bf16),
            pltpu.VMEM((rows_dev, width), bf16),
            pltpu.VMEM((1, width), f32),
            pltpu.VMEM((1, ncols), f32),
            pltpu.VMEM((1, group), jnp.int32),
            pltpu.VMEM((8, group), f32),
            pltpu.VMEM((own_feats, tokens), bf16),
            pltpu.VMEM((n * depth, group), bf16),
            pltpu.VMEM((group, feats), bf16),
            pltpu.VMEM((2, group, width), bf16),
            pltpu.VMEM((2, group, width), bf16),
            pltpu.VMEM((width, ncols), bf16),
            pltpu.VMEM((group, ncols), f32),
            pltpu.VMEM((group, 128), f32),
            pltpu.VMEM((3, group, 128), f32),
            pltpu.VMEM((2, group, 128), f32),
            pltpu.VMEM((2, group, 128), jnp.int32),
            pltpu.VMEM((2, group, TILE), f32),
            pltpu.VMEM((2, group, TILE), bf16),
            pltpu.VMEM((2, n, 8, group), f32),
            pltpu.VMEM((group, 128), f32),
            pltpu.VMEM((group, feats), f32),
            pltpu.VMEM((2, group, ncols), bf16),
            pltpu.VMEM((tokens, own_feats), bf16),
            pltpu.VMEM((line, 2, rows_dev, width), bf16),
            pltpu.VMEM((line, rows_dev, width), bf16),
            pltpu.VMEM((line, rows_dev, width), bf16),
            dma((3,)),
            dma((n, UNIT_PARTS)),
            dma((3,)),
            dma((n, NORM_PARTS)),
            dma,
            dma,
            dma,
            dma,
            dma((2,)),
            dma((2,)),
            dma((2,)),
            dma((2,)),
            dma((2,)),
            dma((2,)),
            dma,
            dma((width // TILE,)),
            dma,
            dma,
            dma((7,)),
            dma((2,)),
            dma((4,)),
            pltpu.SemaphoreType.REGULAR,
        ],
        compiler_params=pltpu.CompilerParams(
            collective_id=0, has_side_effects=True, vmem_limit_bytes=64 * 1024 * 1024 - 65536
        ),
    )(
        hidden.T,
        w_down,
        stream,
        gain,
        vocab,
        vocab_bias.reshape(1, ncols),
        targets.reshape(1, group),
    )

    grad_vocab, grad_input, losses = vocab_call(flipped, dscore, landed, rows, gain, group_losses)
    return (losses.reshape(rows_dev), grad_input, grad_vocab)


def choose(stream, hidden, w_down, final_gain, vocab, vocab_bias, targets):
    rows_dev, width = stream.shape
    group, depth = hidden.shape
    n, groups = lax.axis_size("vp"), lax.axis_size("dp")
    tiles = (
        n % 2 == 0
        and groups == 4
        and rows_dev % 32 == 0
        and depth % (16 * UNIT_PARTS) == 0
        and group % (32 * NORM_PARTS) == 0
        and w_down.shape[1] % 128 == 0
        and width % TILE == 0
        and (width // groups) % 128 == 0
        and vocab.shape[1] % (2 * TILE) == 0
    )
    path = fused if tiles else body
    return path(stream, hidden, w_down, final_gain, vocab, vocab_bias, targets)


def solution(mesh):
    placed = (
        P(("dp", "vp"), None),
        P("dp", "vp"),
        P(None, "vp"),
        P(),
        P(None, "vp"),
        P("vp"),
        P("dp"),
    )
    return jax.shard_map(
        choose,
        mesh=mesh,
        in_specs=placed,
        out_specs=(P(("dp", "vp")), P(("dp", "vp"), None), P("dp", "vp")),
        check_vma=False,
    )
```

```python
import functools

import jax
import jax.numpy as jnp
from jax import lax
from jax.experimental import pallas as pl
from jax.experimental.pallas import tpu as pltpu
from jax.sharding import PartitionSpec as P

norm_eps = 1e-06
zloss_weight = 0.001


def combined_all(value, axis, join):
    pieces = jax.tree.map(lambda part: lax.all_gather(part, axis), value)
    head = jax.tree.map(lambda part: part[0], pieces)
    tail = jax.tree.map(lambda part: part[1:], pieces)
    total, _ = lax.scan(lambda total, section: (join(total, section), None), head, tail)
    return total


def combine_stats(first, second):
    top = jnp.maximum(first[0], second[0])
    total = first[1] * jnp.exp(first[0] - top) + second[1] * jnp.exp(second[0] - top)
    return (top, total, first[2] + second[2])


def body(stream, hidden, w_down, final_gain, vocab, vocab_bias, targets):
    rows_dev = stream.shape[0]
    width = stream.shape[1]
    group = targets.shape[0]
    mine = lax.axis_index("vp")
    feat_cols = w_down.shape[1]
    proj = jnp.dot(
        lax.all_gather(hidden, "vp", axis=1, tiled=True), w_down, preferred_element_type=jnp.float32
    )
    stream_cols = lax.all_to_all(stream, "vp", split_axis=1, concat_axis=0, tiled=True)
    normin_cols = (stream_cols.astype(jnp.float32) + proj).astype(jnp.bfloat16)
    col_values = normin_cols.astype(jnp.float32)
    square_total = lax.psum(jnp.sum(col_values * col_values, axis=1), "vp")
    inv_group = lax.rsqrt(square_total / width + norm_eps)
    gain_cols = lax.dynamic_slice_in_dim(final_gain, mine * feat_cols, feat_cols)
    normed_cols = (col_values * inv_group[:, None] * gain_cols).astype(jnp.bfloat16)
    normed = lax.all_gather(normed_cols, "vp", axis=1, tiled=True)
    normin = lax.all_to_all(normin_cols, "vp", split_axis=0, concat_axis=1, tiled=True)
    values = normin.astype(jnp.float32)
    inv = lax.rsqrt(jnp.mean(values * values, axis=1, keepdims=True) + norm_eps)
    ncols = vocab.shape[1]
    scores = jnp.dot(normed, vocab, preferred_element_type=jnp.float32) + vocab_bias
    local_top = jnp.max(scores, axis=1)
    local_total = jnp.sum(jnp.exp(scores - local_top[:, None]), axis=1)
    column_ids = lax.broadcasted_iota(jnp.int32, (group, ncols), 1) + mine * ncols
    hit = column_ids == targets[:, None]
    local_target = jnp.sum(jnp.where(hit, scores, 0.0), axis=1)
    top, total, target_score = combined_all(
        (local_top, local_total, local_target), "vp", combine_stats
    )
    lse = top + jnp.log(total)
    group_losses = lse - target_score + zloss_weight * lse * lse
    losses = lax.dynamic_slice_in_dim(group_losses, mine * rows_dev, rows_dev)
    probs = jnp.exp(scores - lse[:, None])
    dscore = (probs * (1.0 + 2.0 * zloss_weight * lse)[:, None] - jnp.where(hit, 1.0, 0.0)).astype(
        jnp.bfloat16
    )
    feat_group = width // lax.axis_size("dp")
    feat_start = lax.axis_index("dp") * feat_group
    rows_slice = lax.dynamic_slice_in_dim(
        lax.all_gather(normed, "dp", axis=0, tiled=True), feat_start, feat_group, 1
    )
    grad_vocab = lax.dot_general(
        rows_slice,
        lax.all_gather(dscore, "dp", axis=0, tiled=True),
        (((0,), (0,)), ((), ())),
        preferred_element_type=jnp.float32,
    )
    row_term = lax.dot_general(
        dscore, vocab, (((1,), (1,)), ((), ())), preferred_element_type=jnp.float32
    )
    row_parts = lax.all_to_all(
        row_term[:, None, :].astype(jnp.bfloat16), "vp", split_axis=0, concat_axis=1, tiled=True
    ).astype(jnp.float32)
    dnormed = jnp.sum(row_parts, axis=1)
    scaled = dnormed * final_gain
    grad_input = inv * (
        scaled - values * inv * inv * jnp.mean(values * scaled, axis=1, keepdims=True)
    )
    return (losses, grad_input, grad_vocab)


MESH = pl.DeviceIdType.MESH
UNIT_PARTS = 2
NORM_PARTS = 4
TILE = 512
BLOCK = 512
AHEAD = 4


def send(src, dst, send_sem, recv_sem, vp, dp):
    return pltpu.make_async_remote_copy(
        src_ref=src,
        dst_ref=dst,
        send_sem=send_sem,
        recv_sem=recv_sem,
        device_id={"vp": vp, "dp": dp},
        device_id_type=MESH,
    )


def gather(n, me, dp, parts, own, place, bulk, sems, extra, first, use, between):
    line = n // 2
    here = me // 2
    side = me - 2 * here
    other = me + 1 - 2 * side
    turn = parts // 2
    send_sem, recv_sem = sems
    targets = {0: other, 1: me + 2, 2: me - 2}
    sent = []

    def copy(way, slot, part, src=None):
        return send(
            place(slot, part) if src is None else src,
            place(slot, part),
            send_sem.at[way],
            recv_sem.at[slot, part],
            targets[way],
            dp,
        )

    def holds(conditions, row):
        return functools.reduce(lambda a, b: a & b, [test(row) for test in conditions])

    def when(conditions, action):
        if conditions:
            pl.when(holds(conditions, here))(action)
        else:
            action()

    def put(outer, inner, way, slot, part, src=None):
        when(inner, lambda: copy(way, slot, part, src).start())
        sent.append((outer + inner, way))

    def live(step):
        if step == 0:
            return []
        return [lambda row: (row + step < line) & (row + step >= 0)]

    def ends(step):
        return [lambda row: row + step == (line - 1 if step > 0 else 0)]

    def inside(step):
        return [lambda row: row + step != (line - 1 if step > 0 else 0)]

    up, down = [lambda row: row < line - 1], [lambda row: row > 0]

    for part in range(parts):
        put([], [], 0, me, part, own(part))
        put([], up, 1, me, part, own(part))
        put([], down, 2, me, part, own(part))
        extra(me, part)
    first()

    def straight(k, part, step, way):
        slot = me + 2 * step
        outer = live(step)

        def receive():
            copy(0, slot, part).wait_recv()
            put(outer, up if way == 1 else down, way, slot, part)
            put(outer, inside(step) if part >= turn else [], 0, slot, part)
            extra(slot, part)

        when(outer, receive)

    def routed(k):
        for step, way in ((-k, 1), (k, 2)):
            slot = other + 2 * step
            outer = live(step) + ends(step)

            def receive(slot=slot, outer=outer, way=way):
                for part in range(turn, parts):
                    copy(0, slot, part).wait_recv()
                    put(outer, up if way == 1 else down, way, slot, part)
                    extra(slot, part)

            when(outer, receive)

    def crossed(k):
        for part in range(parts):
            for step in (-k, k) if k else (0,):
                slot = other + 2 * step
                outer = live(step)
                if k and part >= turn:
                    outer = outer + inside(step)

                def receive(slot=slot, part=part):
                    copy(0, slot, part).wait_recv()
                    extra(slot, part)

                when(outer, receive)
                if k == 0 and part >= turn:
                    put([], [lambda row: row == 0] + up, 1, slot, part)
                    put([], [lambda row: row == line - 1] + down, 2, slot, part)

    def used(base, k):
        for step in (-k, k) if k else (0,):
            when(live(step), lambda step=step: use(base + 2 * step))

    for k in range(1, line):
        for part in range(parts):
            straight(k, part, -k, 1)
            straight(k, part, k, 2)
            between(k, part)
        if k > 1:
            routed(k - 1)
        crossed(k - 1)
        used(me, k)
        used(other, k - 1)
    if line > 1:
        routed(line - 1)
    crossed(line - 1)
    used(other, line - 1)

    def finish():
        for way in range(3):
            for row in range(line):
                count = sum(1 for tests, which in sent if which == way and (not tests or holds(tests, row)))
                if count:
                    pl.when(here == row)(lambda: await_bytes(bulk(count), send_sem.at[way]))

    return finish


def await_bytes(ref, sem):
    pltpu.make_async_copy(ref, ref, sem).wait()


def head_kernel(
    n,
    hidden,
    w_down_in,
    stream_in,
    gain_in,
    vocab,
    bias_in,
    targets_in,
    loss_out,
    landed,
    score_out,
    flip_out,
    rows_out,
    w_down,
    stream,
    gain,
    bias,
    targets,
    loss_buf,
    flip_buf,
    units,
    stream_cols,
    normin,
    normed,
    words,
    scores,
    squared,
    lanes,
    lines,
    goal_ids,
    raw,
    stage,
    picked,
    stats,
    goals,
    total,
    dscore,
    slices,
    terms,
    crossing,
    sums,
    unit_send,
    unit_recv,
    norm_send,
    norm_recv,
    stream_send,
    stream_recv,
    twin_send,
    twin_recv,
    stat_send,
    stat_recv,
    score_send,
    score_recv,
    slice_send,
    slice_recv,
    cross_send,
    cross_recv,
    term_send,
    term_recv,
    load_sem,
    keep_sem,
    out_sem,
    twin_ready,
):
    me = lax.axis_index("vp")
    dp = lax.axis_index("dp")
    twin = lax.rem(dp + 2, 4)
    core = lax.rem(dp, 2)
    sibling = dp + 1 - 2 * core
    line = n // 2
    place = me // 2
    side = me - 2 * place
    other = me + 1 - 2 * side
    depth, group = hidden.shape
    width = gain.shape[1]
    feats = stream_cols.shape[1]
    rows_dev = stream.shape[0]
    ncols = bias.shape[1]
    own_feats = slices.shape[1]
    blocks = ncols // TILE
    tiles = width // TILE
    half = group // NORM_PARTS
    piece = depth // UNIT_PARTS

    barrier = pltpu.get_barrier_semaphore()

    above, below = place < line - 1, place > 0

    def greet(vp, home):
        pl.semaphore_signal(barrier, 1, device_id={"vp": vp, "dp": home}, device_id_type=MESH)

    greet(me, twin)
    greet(me, sibling)
    greet(other, dp)
    pl.when(above)(lambda: greet(me + 2, dp))
    pl.when(below)(lambda: greet(me - 2, dp))

    def brought(at, src, dst):
        return pltpu.make_async_copy(src, dst, load_sem.at[at])

    bring = brought(0, hidden, units.at[pl.ds(pl.multiple_of(me * depth, 16), depth), :])
    bring_stream = brought(1, stream_in, stream)
    bring_down = brought(2, w_down_in, w_down)
    bring_targets = brought(3, targets_in, targets)
    bring_gain = brought(4, gain_in, gain)
    bring_bias = brought(5, bias_in, bias)
    load = brought(6, vocab, words)
    for copy in (bring, bring_stream, bring_down, bring_targets, bring_gain, bring_bias, load):
        copy.start()
    pl.semaphore_wait(barrier, 3 + above.astype(jnp.int32) + below.astype(jnp.int32))

    def stream_copy(peer):
        return send(
            stream.at[:, pl.ds(pl.multiple_of(peer * feats, 128), feats)],
            stream_cols.at[pl.ds(pl.multiple_of(me * rows_dev, rows_dev), rows_dev), :],
            stream_send,
            stream_recv,
            peer,
            dp,
        )

    def pair_streams(slot, part):
        if part == 0:
            pl.when((lax.rem(slot, 2) == side) & (slot != me))(lambda: pair_stream(slot))

    def pair_stream(slot):
        stream_copy(slot).start()
        stream_copy(slot + 1 - 2 * side).start()

    def place_units(slot, part):
        return units.at[pl.ds(pl.multiple_of(slot * depth + part * piece, 16), piece), :]

    def product(slot):
        rows = pl.ds(pl.multiple_of(slot * depth, 16), depth)
        return lax.dot_general(
            units[rows, :],
            w_down[rows, :],
            (((0,), (0,)), ((), ())),
            preferred_element_type=jnp.float32,
        )

    def is_goal(j, at, goal):
        ids = lax.broadcasted_iota(jnp.int32, (group, 128), 1) + (me * ncols + j * TILE + at)
        return ids == goal

    def block_cols(j):
        return pl.ds(pl.multiple_of(j * TILE, TILE), TILE)

    def piece_cols(j, i):
        return pl.ds(pl.multiple_of(j * TILE + i * 128, 128), 128)

    def times_vocab(left, t):
        return lax.dot_general(
            left, words[block_cols(t), :], (((1,), (1,)), ((), ())), preferred_element_type=jnp.float32
        )

    def pick_targets(k, part):
        if k == 1 and part == 0:
            load.wait()

        def pick(t, _):
            picked[:, block_cols(t)] = times_vocab(dscore[0], t).astype(jnp.bfloat16)
            return 0

        rounds = min(2, line - 1) * UNIT_PARTS
        at = (k - 1) * UNIT_PARTS + part
        if at < rounds:
            lax.fori_loop(tiles * at // rounds, tiles * (at + 1) // rounds, pick, 0)

    def open_units():
        bring_stream.wait()
        stream_copy(other).start()
        stream_cols[pl.ds(pl.multiple_of(me * rows_dev, rows_dev), rows_dev), :] = stream[
            :, pl.ds(pl.multiple_of(me * feats, 128), feats)
        ]
        bring_targets.wait()
        goals[...] = jnp.transpose(
            jnp.broadcast_to(targets[...].astype(jnp.float32), (128, group))
        )
        goal_ids[0] = goals[...].astype(jnp.int32)

        def mark(j, _):
            for i in range(TILE // 128):
                hit = jnp.where(is_goal(j, 128 * i, goal_ids[0]), 1.0, 0.0)
                dscore[0, :, piece_cols(j, i)] = hit.astype(jnp.bfloat16)
            return 0

        lax.fori_loop(0, blocks, mark, 0)
        bring_down.wait()
        total[...] = product(me)

    def project(slot):
        total[...] += product(slot)

    bring.wait()
    finish_units = gather(
        n,
        me,
        dp,
        UNIT_PARTS,
        lambda part: place_units(me, part),
        place_units,
        lambda count: units.at[pl.ds(0, count * piece), :],
        (unit_send, unit_recv),
        pair_streams,
        open_units,
        project,
        pick_targets,
    )
    streamed = stream_cols.at[pl.ds(0, (n - 1) * rows_dev), :]
    await_bytes(streamed, stream_recv)
    await_bytes(streamed, stream_send)

    pl.semaphore_signal(twin_ready, 1, device_id={"vp": me, "dp": twin}, device_id_type=MESH)

    def cols_of(slot):
        return pl.ds(pl.multiple_of(slot * feats, 128), feats)

    normin[0, :, cols_of(me)] = (stream_cols[...].astype(jnp.float32) + total[...]).astype(jnp.bfloat16)

    def twin_copy(slot, part):
        rows = pl.ds(part * half, half)
        return send(
            normin.at[0, rows, cols_of(slot)],
            normin.at[1, rows, cols_of(slot)],
            twin_send,
            twin_recv,
            me,
            twin,
        )

    def place_norm(slot, part):
        return normin.at[0, pl.ds(part * half, half), cols_of(slot)]

    def folded(pieces, join):
        return functools.reduce(join, pieces)

    def add_squares(slot):
        values = normin[0, :, cols_of(slot)].astype(jnp.float32)
        squares = values * values
        squared[...] += folded([squares[:, at : at + 128] for at in range(0, feats, 128)], jnp.add)

    def open_norm():
        squared[...] = jnp.zeros_like(squared)
        add_squares(me)
        bring_gain.wait()
        bring_bias.wait()
        lanes[0] = jnp.full((group, 128), -jnp.inf, jnp.float32)
        lanes[1] = jnp.zeros((group, 128), jnp.float32)
        lanes[2] = jnp.zeros((group, 128), jnp.float32)

    finish_norm = gather(
        n,
        me,
        dp,
        NORM_PARTS,
        lambda part: place_norm(me, part),
        place_norm,
        lambda count: scores.at[pl.ds(0, count * half // 8), pl.ds(0, 4 * feats)],
        (norm_send, norm_recv),
        lambda slot, part: twin_copy(slot, part).start(),
        open_norm,
        add_squares,
        lambda k, part: None,
    )

    def normalize(which):
        if which == 0:
            mean = jnp.sum(squared[...], axis=1, keepdims=True) / width
            squared[...] = jnp.broadcast_to(lax.rsqrt(mean + norm_eps), (group, 128))

        def block(j, _):
            rows = pl.ds(pl.multiple_of(j * 32, 32), 32)
            values = normin[which, rows, :].astype(jnp.float32)
            if which == 0:
                inv = squared[rows, 0:1]
            else:
                inv = lax.rsqrt(jnp.mean(values * values, axis=1, keepdims=True) + norm_eps)
            normed[which, rows, :] = (values * inv * gain[...]).astype(jnp.bfloat16)
            return 0

        lax.fori_loop(0, group // 32, block, 0)

    def slice_copy(which, home):
        rows = pl.ds(pl.multiple_of(home * group, group), group)
        cols = pl.ds(pl.multiple_of(sibling * own_feats, 128), own_feats)
        return send(
            normed.at[which, :, cols],
            slices.at[rows, :],
            slice_send.at[which],
            slice_recv.at[which],
            me,
            sibling,
        )

    def multiply(which, j, slot):
        raw[slot] = jnp.dot(
            normed[which], words[:, block_cols(j)], preferred_element_type=jnp.float32
        )

    def raw_pieces(j, slot):
        return [
            raw[slot, :, at : at + 128] + bias[:, piece_cols(j, at // 128)]
            for at in range(0, TILE, 128)
        ]

    def pairs(which, absorb, first, last, after=None):
        def body(i, _):
            multiply(which, 2 * i + 1, 1)
            absorb(2 * i, 0)
            multiply(which, 2 * i + 2, 0)
            absorb(2 * i + 1, 1)
            if after:
                after(2 * i)
                after(2 * i + 1)
            return 0

        final = last == blocks // 2
        lax.fori_loop(first, last - 1 if final else last, body, 0)
        if final:
            multiply(which, blocks - 1, 1)
            absorb(blocks - 2, 0)
            if after:
                after(blocks - 2)
            absorb(blocks - 1, 1)
            if after:
                after(blocks - 1)

    def absorb_own(j, slot):
        pieces = raw_pieces(j, slot)
        before = lanes[0]
        peak = jnp.maximum(before, folded(pieces, jnp.maximum))
        powers = [jnp.exp(piece - peak) for piece in pieces]
        for i, piece in enumerate(pieces):
            scores[:, piece_cols(j, i)] = piece
        lanes[0] = peak
        lanes[1] = lanes[1] * jnp.exp(before - peak) + folded(powers, jnp.add)
        hits = [
            jnp.where(is_goal(j, 128 * i, goal_ids[0]), piece, 0.0) for i, piece in enumerate(pieces)
        ]
        lanes[2] += folded(hits, jnp.add)

    def stat_copy(away, j, home):
        peer = lax.rem(me + j, n)
        return send(
            stats.at[0, me],
            stats.at[away, me],
            stat_send.at[away],
            stat_recv.at[away],
            peer,
            home,
        )

    normalize(0)
    slice_copy(0, dp).start()
    multiply(0, 0, 0)
    pairs(0, absorb_own, 0, blocks // 2)
    top = jnp.max(lanes[0], axis=1, keepdims=True)
    weight = jnp.sum(lanes[1] * jnp.exp(lanes[0] - top), axis=1, keepdims=True)
    lanes[0] = jnp.broadcast_to(top, (group, 128))
    lane = lax.broadcasted_iota(jnp.int32, (group, 128), 1)
    packed = jnp.where(
        lane == 0,
        top,
        jnp.where(
            lane == 1,
            weight,
            jnp.where(
                lane == 2,
                jnp.sum(lanes[2], axis=1, keepdims=True),
                jnp.where(lane == 3, goals[...], 0.0),
            ),
        ),
    )
    stats[0, me] = jnp.transpose(packed)[:8, :]

    def start_stats(j, _):
        stat_copy(0, j, dp).start()
        return 0

    def start_away(j, _):
        stat_copy(1, j, twin).start()
        return 0

    lax.fori_loop(1, n, start_stats, 0)
    pl.semaphore_wait(twin_ready, 1)
    lax.fori_loop(0, n, start_away, 0)

    def wait_stats(away):
        arrived = stats.at[away, pl.ds(0, n - 1 + away)]
        await_bytes(arrived, stat_recv.at[away])
        await_bytes(arrived, stat_send.at[away])

    def score_copy(which, home, j):
        rows = pl.ds(pl.multiple_of(home * group, group), group)
        cols = block_cols(j)
        return send(
            dscore.at[which, :, cols],
            score_out.at[rows, cols],
            score_send.at[which],
            score_recv.at[which],
            me,
            sibling,
        )

    def keep_copy(which, home, j):
        rows = pl.ds(pl.multiple_of(home * group, group), group)
        cols = block_cols(j)
        return pltpu.make_async_copy(
            dscore.at[which, :, cols], score_out.at[rows, cols], keep_sem.at[which]
        )

    loss_copy = pltpu.make_async_copy(loss_buf, loss_out, out_sem.at[0])
    flip_copy = pltpu.make_async_copy(flip_buf, flip_out, out_sem.at[1])
    rows_copy = pltpu.make_async_copy(
        normin.at[0, pl.ds(pl.multiple_of(me * rows_dev, rows_dev), rows_dev), :],
        rows_out,
        out_sem.at[2],
    )

    def send_scores(which, home, j):
        score_copy(which, home, j).start()
        keep_copy(which, home, j).start()

    def summary(which):
        parts = stats[which]
        highest = jnp.max(parts[:, 0, :], axis=0, keepdims=True)
        total = jnp.sum(parts[:, 1, :] * jnp.exp(parts[:, 0, :] - highest), axis=0, keepdims=True)
        lse = highest + jnp.log(total)
        if which == 0:
            goal = jnp.sum(parts[:, 2, :], axis=0, keepdims=True)
            loss_buf[...] = jnp.broadcast_to(lse - goal + zloss_weight * lse * lse, (8, group))
            loss_copy.start()
        column = lax.broadcasted_iota(jnp.int32, (128, group), 0)
        turned = jnp.transpose(
            jnp.where(column == 0, lse, jnp.where(column == 1, parts[0, 3:4, :], 0.0))
        )
        lse_col = turned[:, 0:1]
        return lse_col, 1.0 + 2.0 * zloss_weight * lse_col, turned[:, 1:2].astype(jnp.int32)

    def spread(which):
        lse, slope, goal = summary(which)
        lines[0] = jnp.broadcast_to(lse, (group, 128))
        lines[1] = jnp.broadcast_to(slope, (group, 128))
        goal_ids[which] = jnp.broadcast_to(goal, (group, 128))

    def first_terms():
        def power(j, slot):
            for i in range(TILE // 128):
                values = jnp.exp(scores[:, piece_cols(j, i)] - lanes[0]).astype(jnp.bfloat16)
                dscore[0, :, piece_cols(j, i)] = values
                stage[slot, :, i * 128 : (i + 1) * 128] = values

        def accumulate(j, slot):
            raw[0] += lax.dot_general(
                stage[slot],
                words[pl.ds(0, TILE), block_cols(j)],
                (((1,), (1,)), ((), ())),
                preferred_element_type=jnp.float32,
            )

        def body(i, _):
            power(2 * i + 1, 1)
            accumulate(2 * i, 0)
            power(2 * i + 2, 0)
            accumulate(2 * i + 1, 1)
            return 0

        raw[0] = jnp.zeros((group, TILE), jnp.float32)
        power(0, 0)
        lax.fori_loop(0, blocks // 2 - 1, body, 0)
        power(blocks - 1, 1)
        accumulate(blocks - 2, 0)
        accumulate(blocks - 1, 1)

    def derive_own():
        def block(j, _):
            lse, slope, goal = lines[0], lines[1], goal_ids[0]
            for i in range(TILE // 128):
                hit = jnp.where(is_goal(j, 128 * i, goal), 1.0, 0.0)
                power = jnp.exp(scores[:, piece_cols(j, i)] - lse)
                dscore[0, :, piece_cols(j, i)] = (power * slope - hit).astype(jnp.bfloat16)
            return 0

        lax.fori_loop(0, blocks, block, 0)

    def absorb_twin(j, slot):
        lse, slope, goal = lines[0], lines[1], goal_ids[1]
        for i, piece in enumerate(raw_pieces(j, slot)):
            hit = jnp.where(is_goal(j, 128 * i, goal), 1.0, 0.0)
            values = jnp.exp(piece - lse) * slope - hit
            dscore[1, :, piece_cols(j, i)] = values.astype(jnp.bfloat16)


    def cross_copy(t):
        cols = pl.ds(pl.multiple_of(t * TILE, TILE), TILE)
        return send(
            terms.at[:, 1 - side, :, cols],
            crossing.at[:, :, cols],
            cross_send,
            cross_recv.at[t],
            other,
            dp,
        )

    def term_copy(t, j):
        peer = lax.rem(place + j, line)
        cols = pl.ds(pl.multiple_of(t * TILE, TILE), TILE)
        return send(
            sums.at[peer, :, cols],
            landed.at[place, :, cols],
            term_send,
            term_recv,
            2 * peer + side,
            dp,
        )

    def put_terms(t, block):
        for i in range(TILE // 128):
            values = block[:, i * 128 : (i + 1) * 128] * lanes[1]
            values -= picked[:, piece_cols(t, i)].astype(jnp.float32)
            terms[:, :, :, piece_cols(t, i)] = values.astype(jnp.bfloat16).reshape(
                line, 2, rows_dev, 128
            )
        cross_copy(t).start()

    def term_block(t, _):
        put_terms(t, times_vocab(dscore[0], t))
        return 0

    def own_copy(t):
        cols = pl.ds(pl.multiple_of(t * TILE, TILE), TILE)
        return pltpu.make_async_copy(
            sums.at[place, :, cols], landed.at[place, :, cols], out_sem.at[3]
        )

    def pass_on(t):
        cols = pl.ds(t * TILE, TILE)
        cross_copy(t).wait_recv()
        both = terms[:, side, :, cols].astype(jnp.float32) + crossing[:, :, cols].astype(jnp.float32)
        sums[:, :, cols] = both.astype(jnp.bfloat16)
        for j in range(1, line):
            term_copy(t, j).start()
        own_copy(t).start()

    rows_copy.start()
    first_terms()
    raw[1] = times_vocab(dscore[0], 1)
    await_bytes(normin.at[1], twin_recv)
    await_bytes(normin.at[1], twin_send)
    normalize(1)
    slice_copy(1, twin).start()
    wait_stats(0)
    spread(0)
    lanes[1] = jnp.exp(lanes[0] - lines[0]) * lines[1]
    put_terms(0, raw[0])
    put_terms(1, raw[1])
    lax.fori_loop(2, tiles, term_block, 0)

    def release(first, last):
        for i in range(blocks // 2 * first // 4, blocks // 2 * last // 4):
            send_scores(0, dp, 2 * i)
            send_scores(0, dp, 2 * i + 1)

    def turn_slices():
        for which, home in ((0, dp), (1, twin)):
            rows = pl.ds(pl.multiple_of(home * group, group), group)
            own_cols = pl.ds(pl.multiple_of(dp * own_feats, 128), own_feats)
            slices[rows, :] = normed[which, :, own_cols]
            slice_copy(which, home).wait()
        flip_buf[...] = jnp.transpose(slices[...])
        flip_copy.start()

    def score_twin(first, last):
        pairs(1, absorb_twin, first, last, lambda j: send_scores(1, twin, j))

    pieces = blocks // 2
    derive_own()
    wait_stats(1)
    spread(1)
    multiply(1, 0, 0)
    for t in range(tiles):
        if t == tiles - 1:
            turn_slices()
        pass_on(t)
        if t < 2:
            release(2 * t, 2 * t + 2)
            score_twin(pieces * t // 4, pieces * (t + 1) // 4)
    score_twin(pieces // 2, pieces)
    passed = sums.at[pl.ds(0, line - 1)]
    await_bytes(passed, term_recv)
    await_bytes(passed, term_send)
    await_bytes(crossing, cross_send)
    await_bytes(sums.at[0], out_sem.at[3])
    for which in range(2):
        await_bytes(dscore.at[which], keep_sem.at[which])
        await_bytes(dscore.at[which], score_send.at[which])
        await_bytes(dscore.at[which], score_recv.at[which])
    finish_units()
    finish_norm()
    loss_copy.wait()
    flip_copy.wait()
    rows_copy.wait()


def vocab_kernel(
    flipped_in,
    dscore_in,
    landed_in,
    rows_in,
    gain_in,
    losses_in,
    vocab_out,
    input_out,
    loss_out,
    flipped,
    dscore,
    results,
    landed,
    rows,
    gain,
    inputs,
    losses,
    loss_row,
    load_sem,
    block_sem,
    out_sem,
    tail_sem,
):
    rows_dev = loss_row.shape[1]
    group = losses.shape[1]
    count = dscore.shape[0]

    def block_in(j):
        cols = pl.ds(pl.multiple_of(j * BLOCK, BLOCK), BLOCK)
        return pltpu.make_async_copy(dscore_in.at[:, cols], dscore.at[j], block_sem.at[j])

    def block_out(j):
        cols = pl.ds(pl.multiple_of(j * BLOCK, BLOCK), BLOCK)
        return pltpu.make_async_copy(results.at[j], vocab_out.at[:, cols], out_sem.at[j])

    loads = [
        pltpu.make_async_copy(src, dst, load_sem.at[i])
        for i, (src, dst) in enumerate(
            [
                (flipped_in, flipped),
                (landed_in, landed),
                (rows_in, rows),
                (gain_in, gain),
                (losses_in, losses),
            ]
        )
    ]
    put_input = pltpu.make_async_copy(inputs, input_out, tail_sem.at[0])
    put_losses = pltpu.make_async_copy(loss_row, loss_out, tail_sem.at[1])
    loads[0].start()
    block_in(0).start()
    for load in loads[1:]:
        load.start()
    for j in range(1, min(AHEAD, count)):
        block_in(j).start()

    def multiply(j, _):
        @pl.when(j + AHEAD - 1 < count)
        def _():
            block_in(j + AHEAD - 1).start()

        block_in(j).wait()
        results[j] = jnp.dot(flipped[...], dscore[j], preferred_element_type=jnp.float32)
        block_out(j).start()
        return 0

    for load in loads:
        load.wait()
    block_in(0).wait()
    results[0] = jnp.dot(flipped[...], dscore[0], preferred_element_type=jnp.float32)
    values = rows[...].astype(jnp.float32)
    inv = lax.rsqrt(jnp.mean(values * values, axis=1, keepdims=True) + norm_eps)
    dnormed = landed[0].astype(jnp.float32)
    for slot in range(1, landed.shape[0]):
        dnormed += landed[slot].astype(jnp.float32)
    scaled = dnormed * gain[...]
    inputs[...] = inv * (
        scaled - values * inv * inv * jnp.mean(values * scaled, axis=1, keepdims=True)
    )
    shift = lax.rem(group - lax.axis_index("vp") * rows_dev, group)
    loss_row[...] = pltpu.roll(losses[...], shift, 1)[0:1, :rows_dev]
    block_out(0).start()
    put_input.start()
    put_losses.start()

    def finish(j, _):
        block_out(j).wait()
        return 0

    lax.fori_loop(1, count, multiply, 0)
    put_input.wait()
    put_losses.wait()
    lax.fori_loop(0, count, finish, 0)


def vocab_call(flipped, dscore, landed, rows, gain, group_losses):
    own_feats, tokens = flipped.shape
    ncols = dscore.shape[1]
    line, rows_dev, width = landed.shape
    group = group_losses.shape[1]
    f32, bf16 = jnp.float32, jnp.bfloat16
    dma = pltpu.SemaphoreType.DMA
    hbm = pl.BlockSpec(memory_space=pl.ANY)
    count = ncols // BLOCK
    return pl.pallas_call(
        vocab_kernel,
        out_shape=(
            jax.ShapeDtypeStruct((own_feats, ncols), f32),
            jax.ShapeDtypeStruct((rows_dev, width), f32),
            jax.ShapeDtypeStruct((1, rows_dev), f32),
        ),
        in_specs=[hbm] * 6,
        out_specs=(hbm,) * 3,
        scratch_shapes=[
            pltpu.VMEM((own_feats, tokens), bf16),
            pltpu.VMEM((count, tokens, BLOCK), bf16),
            pltpu.VMEM((count, own_feats, BLOCK), f32),
            pltpu.VMEM((line, rows_dev, width), bf16),
            pltpu.VMEM((rows_dev, width), bf16),
            pltpu.VMEM((1, width), f32),
            pltpu.VMEM((rows_dev, width), f32),
            pltpu.VMEM((8, group), f32),
            pltpu.VMEM((1, rows_dev), f32),
            dma((5,)),
            dma((count,)),
            dma((count,)),
            dma((2,)),
        ],
        compiler_params=pltpu.CompilerParams(vmem_limit_bytes=64 * 1024 * 1024 - 65536),
    )(flipped, dscore, landed, rows, gain, group_losses)


def fused(stream, hidden, w_down, final_gain, vocab, vocab_bias, targets):
    n = lax.axis_size("vp")
    groups = lax.axis_size("dp")
    rows_dev, width = stream.shape
    group, depth = hidden.shape
    feats = w_down.shape[1]
    ncols = vocab.shape[1]
    own_feats = width // groups
    tokens = groups * group
    line = n // 2
    f32, bf16 = jnp.float32, jnp.bfloat16
    dma = pltpu.SemaphoreType.DMA
    hbm = pl.BlockSpec(memory_space=pl.ANY)
    gain = final_gain.reshape(1, width)
    group_losses, landed, dscore, flipped, rows = pl.pallas_call(
        functools.partial(head_kernel, n),
        out_shape=(
            jax.ShapeDtypeStruct((8, group), f32),
            jax.ShapeDtypeStruct((line, rows_dev, width), bf16),
            jax.ShapeDtypeStruct((tokens, ncols), bf16),
            jax.ShapeDtypeStruct((own_feats, tokens), bf16),
            jax.ShapeDtypeStruct((rows_dev, width), bf16),
        ),
        in_specs=[hbm] * 7,
        out_specs=(hbm,) * 5,
        scratch_shapes=[
            pltpu.VMEM(w_down.shape, bf16),
            pltpu.VMEM((rows_dev, width), bf16),
            pltpu.VMEM((1, width), f32),
            pltpu.VMEM((1, ncols), f32),
            pltpu.VMEM((1, group), jnp.int32),
            pltpu.VMEM((8, group), f32),
            pltpu.VMEM((own_feats, tokens), bf16),
            pltpu.VMEM((n * depth, group), bf16),
            pltpu.VMEM((group, feats), bf16),
            pltpu.VMEM((2, group, width), bf16),
            pltpu.VMEM((2, group, width), bf16),
            pltpu.VMEM((width, ncols), bf16),
            pltpu.VMEM((group, ncols), f32),
            pltpu.VMEM((group, 128), f32),
            pltpu.VMEM((3, group, 128), f32),
            pltpu.VMEM((2, group, 128), f32),
            pltpu.VMEM((2, group, 128), jnp.int32),
            pltpu.VMEM((2, group, TILE), f32),
            pltpu.VMEM((2, group, TILE), bf16),
            pltpu.VMEM((group, width), bf16),
            pltpu.VMEM((2, n, 8, group), f32),
            pltpu.VMEM((group, 128), f32),
            pltpu.VMEM((group, feats), f32),
            pltpu.VMEM((2, group, ncols), bf16),
            pltpu.VMEM((tokens, own_feats), bf16),
            pltpu.VMEM((line, 2, rows_dev, width), bf16),
            pltpu.VMEM((line, rows_dev, width), bf16),
            pltpu.VMEM((line, rows_dev, width), bf16),
            dma((3,)),
            dma((n, UNIT_PARTS)),
            dma((3,)),
            dma((n, NORM_PARTS)),
            dma,
            dma,
            dma,
            dma,
            dma((2,)),
            dma((2,)),
            dma((2,)),
            dma((2,)),
            dma((2,)),
            dma((2,)),
            dma,
            dma((width // TILE,)),
            dma,
            dma,
            dma((7,)),
            dma((2,)),
            dma((4,)),
            pltpu.SemaphoreType.REGULAR,
        ],
        compiler_params=pltpu.CompilerParams(
            collective_id=0, has_side_effects=True, vmem_limit_bytes=64 * 1024 * 1024 - 65536
        ),
    )(
        hidden.T,
        w_down,
        stream,
        gain,
        vocab,
        vocab_bias.reshape(1, ncols),
        targets.reshape(1, group),
    )

    grad_vocab, grad_input, losses = vocab_call(flipped, dscore, landed, rows, gain, group_losses)
    return (losses.reshape(rows_dev), grad_input, grad_vocab)


def choose(stream, hidden, w_down, final_gain, vocab, vocab_bias, targets):
    rows_dev, width = stream.shape
    group, depth = hidden.shape
    n, groups = lax.axis_size("vp"), lax.axis_size("dp")
    tiles = (
        n % 2 == 0
        and n >= 4
        and groups == 4
        and rows_dev % 32 == 0
        and depth % (16 * UNIT_PARTS) == 0
        and group % (32 * NORM_PARTS) == 0
        and w_down.shape[1] % 128 == 0
        and width % TILE == 0
        and width >= 4 * TILE
        and (width // groups) % 128 == 0
        and vocab.shape[1] % (8 * TILE) == 0
    )
    path = fused if tiles else body
    return path(stream, hidden, w_down, final_gain, vocab, vocab_bias, targets)


def solution(mesh):
    placed = (
        P(("dp", "vp"), None),
        P("dp", "vp"),
        P(None, "vp"),
        P(),
        P(None, "vp"),
        P("vp"),
        P("dp"),
    )
    return jax.shard_map(
        choose,
        mesh=mesh,
        in_specs=placed,
        out_specs=(P(("dp", "vp")), P(("dp", "vp"), None), P("dp", "vp")),
        check_vma=False,
    )
```
